256 devices in a mesh: ep: 64 (over z, y, core), tp: 4 (over x).
Axes of the slice: x: 4, y: 4, z: 8, core: 2. Of those that a mesh axis runs over, the one named last changes fastest.
Arguments:
- tokens: bfloat16 [1536, 1024], P('ep'), may hold values from -1.796875 to 1.796875
- attn_gain: float32 [1024], replicated, may hold values from 0.1 to 1.9
- w_query: bfloat16 [1024, 1024], P(None, 'tp'), may hold values from -0.1875 to 0.1875
- w_key: bfloat16 [1024, 256], P(None, 'tp'), may hold values from -0.1875 to 0.1875
- w_value: bfloat16 [1024, 256], P(None, 'tp'), may hold values from -0.1875 to 0.1875
- w_forget: bfloat16 [1024, 4], P(None, 'tp'), may hold values from -0.1875 to 0.1875
- forget_bias: float32 [4], P('tp'), may hold values from -1 to 2
- query_gain: float32 [64], replicated, may hold values from 0.1 to 1.9
- key_gain: float32 [64], replicated, may hold values from 0.1 to 1.9
- cache_pairs: bfloat16 [1536, 4, 1024, 128], P('ep', 'tp'), may hold values from -6 to 206
- cache_cum: float32 [1536, 4, 1024], P('ep', 'tp'), may hold values from -1024 to 0, as said below
- lengths: int32 [1536], P('ep'), may hold values from 64 to 1024, as said below
- w_output: bfloat16 [1024, 1024], P('tp'), may hold values from -0.1875 to 0.1875
- ffn_gain: float32 [1024], replicated, may hold values from 0.1 to 1.9
- expert_ids: int32 [1536, 2], replicated, may hold values from 0 to 63, all different within a row; in each aligned block of 24 rows (0 to 23, 24 to 47, ...) at most 2 rows name the same one
- route_weight: float32 [1536, 2], replicated, may hold values from 0.2 to 1
- w_exp_gate: bfloat16 [64, 1024, 3584], P('ep', None, 'tp'), may hold values from -0.1875 to 0.1875
- w_exp_up: bfloat16 [64, 1024, 3584], P('ep', None, 'tp'), may hold values from -0.1875 to 0.1875
- w_exp_down: bfloat16 [64, 3584, 1024], P('ep', 'tp'), may hold values from -0.09375 to 0.09375
- shared_gate: bfloat16 [1024], replicated, may hold values from -0.1875 to 0.1875
- w_dense_gate: bfloat16 [4096, 1024], P('ep'), may hold values from -0.1875 to 0.1875
- w_dense_up: bfloat16 [4096, 1024], P('ep'), may hold values from -0.1875 to 0.1875
- w_dense_down: bfloat16 [4096, 1024], P('ep', 'tp'), may hold values from -0.09375 to 0.09375
Outputs:
- layer_out: bfloat16 [1536, 1024], P('ep', 'tp')
The draws below stay inside these ranges and needn't reach their ends.
Inputs may be any that keep to these rules, and one draw needn't show every extreme that they name: The cache of sequence b holds positions 0 to lengths[b] - 1; some sequence has 1024. `expert_ids`: each row names 2 different experts; in each aligned block of 24 rows no expert is named by more than 2 rows. cache_cum[b, g, s] never rises with s.
All inputs are finite; a program needn't handle non-finite values.
Results may differ from the reference program's by a relative error of at most 0.02.
Values may be sent and summed in bfloat16 or wider, within the bound.
A program may use at most 64 MiB of HBM per device.

```python
import math
import jax
import jax.numpy as jnp
import numpy as np
from jax import lax

D = 1024
HEADS = 16
HEAD_DIM = 64
KV_HEADS = 4
FF_EXPERT = 3584
DENSE_FF = 4096
TOP_K = 2
SEQ_GRP = 24
CACHE_SLOTS = 1024
BATCH = 1536
EXPERTS = 64
CAP = 2
HEAD_GROUP = 4
N_EP = 64
N_TP = 4


def draw_lengths(key, part):
    lengths_drawn = jax.random.randint(key, (BATCH,), CACHE_SLOTS // 16, CACHE_SLOTS + 1, dtype=jnp.int32)
    return lengths_drawn.at[0].set(CACHE_SLOTS)


def draw_cache_pairs(key, part):
    base_key = jax.random.fold_in(key, 0)
    complete_shape = (BATCH, KV_HEADS, CACHE_SLOTS, 2 * HEAD_DIM)
    entries = jnp.clip(jax.random.normal(base_key, complete_shape, jnp.float32), -6.0, 6.0)
    return entries.astype(jnp.bfloat16)


def draw_cache_cum(key, part):
    key_sequence = jax.random.split(key, 8)
    complete_shape = (BATCH, KV_HEADS, CACHE_SLOTS)
    head_shape = (BATCH, KV_HEADS, 1)
    slow_share = 0.5
    sluggish_flag = jax.random.uniform(key_sequence[0], head_shape) < slow_share
    whole_rate = jnp.exp(jax.random.uniform(key_sequence[1], head_shape, jnp.float32, jnp.log(0.4), jnp.log(2.0))) / CACHE_SLOTS
    quick_rate = 1.0 / jax.random.uniform(key_sequence[2], head_shape, jnp.float32, 30.0, 50.0)
    step_frequency = jnp.where(sluggish_flag, whole_rate, quick_rate)
    device_multiplier = jnp.exp(jax.random.uniform(key_sequence[3], head_shape, jnp.float32, jnp.log(0.5), jnp.log(2.0)))
    block_multiplier = jnp.exp(jax.random.uniform(key_sequence[4], (BATCH, KV_HEADS, 8), jnp.float32, jnp.log(0.5), jnp.log(2.0)))
    block_multiplier = jnp.repeat(block_multiplier, CACHE_SLOTS // 8, axis=2)
    coarse_multiplier = jax.random.uniform(key_sequence[5], complete_shape, jnp.float32, 0.5, 2.0)
    spike_flag = (jax.random.uniform(key_sequence[6], complete_shape) < 3.0 / CACHE_SLOTS) & sluggish_flag
    spike_penalty = jnp.log(jax.random.uniform(key_sequence[7], complete_shape, jnp.float32, 0.5, 0.8))
    gate_logarithms = -step_frequency * device_multiplier * block_multiplier * coarse_multiplier + jnp.where(spike_flag, spike_penalty, 0.0)
    return jnp.cumsum(gate_logarithms, axis=2)


def block_levels(key, shape, shards, smallest, high):
    loudness, own = 1.0, jax.random.fold_in(key, 6)
    for axis_at, parts in shards:
        heights = jnp.exp(jax.random.uniform(jax.random.fold_in(own, axis_at), (parts,), jnp.float32, smallest / len(shards), high / len(shards)))
        loudness = loudness * jnp.repeat(heights, shape[axis_at] // parts).reshape([-1 if axis == axis_at else 1 for axis in range(len(shape))])
    return loudness


def routed_block(stream_key, own, number, rows, amount, top, reach, slope):
    sequence = jax.random.permutation(stream_key, amount)
    crowded, common = shares(amount, rows * top, reach, slope, True), shares(amount, rows * top, reach, slope, False)
    places = jnp.arange(amount)

    def named(sizes, rotation):
        used = int((sizes > 0).sum())
        fixed = max(1, used // 4)
        shifted = fixed + (places - fixed + rotation * (used - fixed)) % max(1, amount - fixed)
        return jnp.zeros((amount,), jnp.int32).at[sequence[jnp.where(places < fixed, places, shifted)]].set(jnp.asarray(sizes, jnp.int32))

    sizes = jnp.where(number % 4 == 0, named(crowded, number // 4), named(common, number - number // 4 - 1))
    mixed = jax.random.permutation(jax.random.fold_in(own, 3), amount)
    giver, taker = mixed[0:amount // 2 * 2:2], mixed[1:amount // 2 * 2:2]
    slack = jnp.minimum(sizes[giver] - 1, reach - sizes[taker]) // 2
    slack = jnp.where((giver == sequence[0]) | (taker == sequence[0]) | (sizes[taker] == 0), 0, jnp.maximum(slack, 0))
    shifted = jax.random.randint(jax.random.fold_in(own, 4), (amount // 2,), 0, 1 << 20) % (slack + 1)
    sizes = sizes.at[giver].add(-shifted).at[taker].add(shifted)
    members = jnp.searchsorted(jnp.cumsum(sizes), jnp.arange(rows * top), side="right").astype(jnp.int32)
    listing = members.reshape(top, rows).T
    listing = listing[jax.random.permutation(jax.random.fold_in(own, 1), rows)]
    rotation = jax.random.randint(jax.random.fold_in(own, 2), (rows, 1), 0, top)
    return jnp.take_along_axis(listing, (jnp.arange(top)[None, :] + rotation) % top, axis=1)


def shares(number_of, total, reach, lean, full):
    weights = [(1 << 20) // math.isqrt(rank ** lean) + 1 for rank in range(1, number_of + 1)]
    largest = reach if full else min(reach, max(-(-total // number_of), total * weights[0] // sum(weights)))
    least = 1 if total - largest >= number_of - 1 else 0
    given, spare = [largest] + [least] * (number_of - 1), total - largest - least * (number_of - 1)
    while spare > 0:
        candidates = [i for i in range(1, number_of) if given[i] < largest] or [i for i in range(1, number_of) if given[i] < reach]
        whole, budget = sum([weights[i] for i in candidates]), spare
        for i in candidates:
            extra = min(reach - given[i], max(1, budget * weights[i] // whole), spare)
            given[i] = given[i] + extra
            spare = spare - extra
    return np.array(given)


def bell_draw(rng, extent, scale, most, shards=(), held_as=jnp.bfloat16):
    gain = block_levels(rng, extent, shards, -0.22, 0.18) if shards else 1.0
    result = jax.random.normal(rng, extent, jnp.float32) * scale * gain
    return jnp.minimum(jnp.maximum(result, -most), most).astype(held_as)


def setup_inputs(seed: int = 0) -> dict:
    keys = jax.random.split(jax.random.key(seed), 24)
    tokens = bell_draw(keys[0], (BATCH, D), 0.3, 1.796875, ((0, 64),))
    attn_gain = jnp.clip(1.0 + 0.18 * jax.random.normal(keys[1], (D,), jnp.float32), 0.1, 1.9)
    w_query = bell_draw(keys[2], (D, HEADS * HEAD_DIM), D ** -0.5, 0.1875, ((1, 4),))
    w_key = bell_draw(keys[3], (D, KV_HEADS * HEAD_DIM), D ** -0.5, 0.1875, ((1, 4),))
    w_value = bell_draw(keys[4], (D, KV_HEADS * HEAD_DIM), D ** -0.5, 0.1875, ((1, 4),))
    w_forget = bell_draw(keys[5], (D, KV_HEADS), D ** -0.5, 0.1875, ((1, 4),))
    forget_bias = jnp.clip(-1.0 + 3.0 * jax.random.uniform(keys[6], (KV_HEADS,), jnp.float32) ** block_levels(keys[6], (KV_HEADS,), ((0, 4),), -0.2, 0.2), -1.0, 2.0)
    query_gain = jnp.clip(1.0 + 0.18 * jax.random.normal(keys[7], (HEAD_DIM,), jnp.float32), 0.1, 1.9)
    key_gain = jnp.clip(1.0 + 0.18 * jax.random.normal(keys[8], (HEAD_DIM,), jnp.float32), 0.1, 1.9)
    cache_pairs = draw_cache_pairs(jax.random.fold_in(keys[23], 71), 0)
    cache_cum = draw_cache_cum(jax.random.fold_in(keys[23], 71), 0)
    lengths = draw_lengths(jax.random.fold_in(keys[23], 71), 0)
    w_output = bell_draw(keys[12], (HEADS * HEAD_DIM, D), (HEADS * HEAD_DIM) ** -0.5, 0.1875, ((0, 4),))
    ffn_gain = jnp.clip(1.0 + 0.18 * jax.random.normal(keys[13], (D,), jnp.float32), 0.1, 1.9)
    expert_ids_keys = jax.random.split(jax.random.fold_in(keys[14], 1), BATCH // SEQ_GRP)
    expert_ids_turns = jax.random.permutation(jax.random.fold_in(keys[14], 3), BATCH // SEQ_GRP)
    expert_ids = jax.vmap(lambda own, number: routed_block(jax.random.fold_in(keys[14], 2), own, number, SEQ_GRP, EXPERTS, TOP_K, CAP, 2))(expert_ids_keys, expert_ids_turns).reshape((BATCH, TOP_K))
    route_weight = jnp.clip(jax.random.uniform(keys[15], (BATCH, TOP_K), jnp.float32, 0.2, 1.0), 0.2, 1.0)
    w_exp_gate = bell_draw(keys[16], (EXPERTS, D, FF_EXPERT), D ** -0.5, 0.1875, ((0, 64), (2, 4)))
    w_exp_up = bell_draw(keys[17], (EXPERTS, D, FF_EXPERT), D ** -0.5, 0.1875, ((0, 64), (2, 4)))
    w_exp_down = bell_draw(keys[18], (EXPERTS, FF_EXPERT, D), FF_EXPERT ** -0.5, 0.09375, ((0, 64), (1, 4)))
    shared_gate = bell_draw(keys[19], (D,), D ** -0.5, 0.1875)
    w_dense_gate = bell_draw(keys[20], (DENSE_FF, D), D ** -0.5, 0.1875, ((0, 64),))
    w_dense_up = bell_draw(keys[21], (DENSE_FF, D), D ** -0.5, 0.1875, ((0, 64),))
    w_dense_down = bell_draw(keys[22], (DENSE_FF, D), DENSE_FF ** -0.5, 0.09375, ((0, 64), (1, 4)))
    return dict(tokens=tokens, attn_gain=attn_gain, w_query=w_query, w_key=w_key, w_value=w_value, w_forget=w_forget, forget_bias=forget_bias, query_gain=query_gain, key_gain=key_gain, cache_pairs=cache_pairs, cache_cum=cache_cum, lengths=lengths, w_output=w_output, ffn_gain=ffn_gain, expert_ids=expert_ids, route_weight=route_weight, w_exp_gate=w_exp_gate, w_exp_up=w_exp_up, w_exp_down=w_exp_down, shared_gate=shared_gate, w_dense_gate=w_dense_gate, w_dense_up=w_dense_up, w_dense_down=w_dense_down)


EPSILON = 1e-06

def rms_scale(values, gain_row):
    mean_square = lax.optimization_barrier(jnp.mean(values * values, axis=-1, keepdims=True))
    return values * lax.rsqrt(mean_square + EPSILON) * gain_row

def stored(values):
    return lax.optimization_barrier(values.astype(jnp.bfloat16))

def rounded(values):
    return stored(values).astype(jnp.float32)

def attend(per_block):
    query_rows, fresh_key, value_new, now_cum, cache_block, cum_block, length = per_block
    head_size = query_rows.shape[-1]
    position = jnp.arange(cache_block.shape[2], dtype=jnp.int32)
    is_live = position[None, None, :] < length[:, None, None]
    cached_keys = cache_block[..., :head_size].astype(jnp.float32)
    cached_values = cache_block[..., head_size:].astype(jnp.float32)
    score_multiplier = head_size ** (-0.5)
    past_score = jnp.einsum('bkgd,bkld->bkgl', query_rows, cached_keys) * score_multiplier
    past_score = past_score + (now_cum[:, :, None] - cum_block)[:, :, None, :]
    past_score = jnp.where(is_live[:, :, None, :], past_score, -jnp.inf)
    current_score = jnp.einsum('nlte,nle->nlt', query_rows, fresh_key) * score_multiplier
    row_peak = jnp.maximum(lax.optimization_barrier(jnp.max(past_score, axis=3)), current_score)
    past_exp = jnp.exp(past_score - row_peak[..., None])
    own_exp = jnp.exp(current_score - row_peak)
    denom_sum = lax.optimization_barrier(jnp.sum(past_exp, axis=3)) + own_exp
    past_prob = rounded(past_exp / denom_sum[..., None])
    own_prob = rounded(own_exp / denom_sum)
    head_mix = jnp.einsum('bkgl,bkld->bkgd', past_prob, cached_values)
    head_mix = head_mix + own_prob[..., None] * value_new[:, :, None, :]
    return stored(head_mix)

def reference(tokens, attn_gain, w_query, w_key, w_value, w_forget, forget_bias, query_gain, key_gain, cache_pairs, cache_cum, lengths, w_output, ffn_gain, expert_ids, route_weight, w_exp_gate, w_exp_up, w_exp_down, shared_gate, w_dense_gate, w_dense_up, w_dense_down):
    tokens_f = tokens.astype(jnp.float32)
    normed = stored(rms_scale(tokens_f, attn_gain))
    group_size = HEADS // KV_HEADS
    query_raw = jnp.dot(normed, w_query, preferred_element_type=jnp.float32)
    query_rows = rounded(rms_scale(query_raw.reshape(BATCH, KV_HEADS, group_size, HEAD_DIM), query_gain))
    key_raw = jnp.dot(normed, w_key, preferred_element_type=jnp.float32).reshape(BATCH, KV_HEADS, HEAD_DIM)
    fresh_key = rounded(rms_scale(key_raw, key_gain))
    value_new = rounded(jnp.dot(normed, w_value, preferred_element_type=jnp.float32))
    value_new = value_new.reshape(BATCH, KV_HEADS, HEAD_DIM)
    log_gate = jax.nn.log_sigmoid(jnp.dot(normed, w_forget, preferred_element_type=jnp.float32) + forget_bias)
    last_index = jnp.broadcast_to((lengths - 1)[:, None, None], (BATCH, KV_HEADS, 1)).astype(jnp.int32)
    last_cum = jnp.take_along_axis(cache_cum, last_index, axis=2)[:, :, 0]
    now_cum = last_cum + log_gate

    def to_blocks(values):
        return values.reshape((N_EP, SEQ_GRP) + values.shape[1:])
    head_mix = lax.map(attend, tuple((to_blocks(item) for item in (query_rows, fresh_key, value_new, now_cum, cache_pairs, cache_cum, lengths))))
    head_mix = head_mix.reshape(BATCH, HEADS * HEAD_DIM)
    head_span = HEAD_GROUP * HEAD_DIM
    attn_out = jnp.zeros((BATCH, D), jnp.float32)
    for member in range(N_TP):
        partial_value = jnp.dot(head_mix[:, member * head_span:(member + 1) * head_span], w_output[member * head_span:(member + 1) * head_span], preferred_element_type=jnp.float32)
        attn_out = attn_out + rounded(partial_value)
    residual = stored(tokens_f + attn_out)
    residual_f = residual.astype(jnp.float32)
    normed_two = stored(rms_scale(residual_f, ffn_gain))
    grouped_f = normed_two.astype(jnp.float32).reshape(N_EP, SEQ_GRP, D)
    gate_raw = jnp.dot(normed_two, w_dense_gate.T, preferred_element_type=jnp.float32)
    up_raw = jnp.dot(normed_two, w_dense_up.T, preferred_element_type=jnp.float32)
    dense_hidden = stored(jax.nn.silu(gate_raw) * up_raw)
    mix_gate = jax.nn.sigmoid(jnp.dot(normed_two, shared_gate, preferred_element_type=jnp.float32))
    dense_out = mix_gate[:, None] * jnp.dot(dense_hidden, w_dense_down, preferred_element_type=jnp.float32)
    unit_span = FF_EXPERT // N_TP

    def expert_step(running, expert_item):
        member_id, gate_w, up_w, down_w = expert_item
        chosen = expert_ids == member_id
        is_hit = lax.optimization_barrier(jnp.sum(chosen.astype(jnp.int32), axis=1)).reshape(N_EP, SEQ_GRP)
        weight = lax.optimization_barrier(jnp.sum(jnp.where(chosen, route_weight, 0.0), axis=1))
        slot_rank = jnp.cumsum(is_hit, axis=1)
        slot_ids = jnp.arange(1, CAP + 1, dtype=jnp.int32)[None, :, None]
        picker = ((slot_rank[:, None, :] == slot_ids) & (is_hit[:, None, :] == 1)).astype(jnp.float32)
        picked = jnp.einsum('scn,snd->scd', picker, grouped_f).reshape(N_EP * CAP, D).astype(jnp.bfloat16)
        gate_part = jnp.dot(picked, gate_w, preferred_element_type=jnp.float32)
        up_part = jnp.dot(picked, up_w, preferred_element_type=jnp.float32)
        hidden = stored(jax.nn.silu(gate_part) * up_part)
        expert_rows = jnp.zeros((N_EP * CAP, D), jnp.float32)
        for member in range(N_TP):
            partial_value = jnp.dot(hidden[:, member * unit_span:(member + 1) * unit_span], down_w[member * unit_span:(member + 1) * unit_span], preferred_element_type=jnp.float32)
            expert_rows = expert_rows + rounded(partial_value)
        expert_rows = rounded(expert_rows).reshape(N_EP, CAP, D)
        placed = jnp.einsum('scn,scd->snd', picker, expert_rows).reshape(BATCH, D)
        return (running + placed * weight[:, None], None)
    expert_sum = lax.scan(expert_step, jnp.zeros((BATCH, D), jnp.float32), (jnp.arange(EXPERTS, dtype=jnp.int32), w_exp_gate, w_exp_up, w_exp_down))[0]
    return (residual_f + expert_sum + dense_out).astype(jnp.bfloat16)
```

```python
import functools

import jax
import jax.numpy as jnp
from jax import lax
from jax.experimental import pallas as pl
from jax.experimental.pallas import tpu as pltpu
from jax.sharding import PartitionSpec as P

EPSILON = 1e-06
MESH = pl.DeviceIdType.MESH
BF = jnp.bfloat16
F32 = jnp.float32
GROUP = 8
NEG = -1e30


def iota(shape, dim):
    return lax.broadcasted_iota(jnp.int32, shape, dim)


def dot(a, b):
    return jnp.dot(a, b, preferred_element_type=F32)


def dot_nt(a, b):
    return lax.dot_general(a, b, (((1,), (1,)), ((), ())), preferred_element_type=F32)


def rms(values):
    return lax.rsqrt(jnp.mean(values * values, axis=-1, keepdims=True) + EPSILON)


def silu(v):
    return v / (1.0 + jnp.exp(-v))


def one_hot(cond):
    return jnp.where(cond, 1.0, 0.0).astype(BF)


def kernel(
    n_ep,
    n_tp,
    tokens_h,
    attn_gain_h,
    w_query_h,
    w_key_h,
    w_value_h,
    w_forget_h,
    forget_bias_h,
    query_gain_h,
    key_gain_h,
    cache_h,
    cum_h,
    lengths_h,
    w_output_h,
    ffn_gain_h,
    ids_h,
    route_h,
    w_gate_h,
    w_up_h,
    w_down_h,
    shared_gate_h,
    dense_gate_h,
    dense_up_h,
    dense_down_h,
    out_ref,
    tok,
    again,
    wq,
    wk,
    wv,
    wf,
    fb,
    qg,
    kg,
    cache,
    cum,
    lens,
    wo,
    fgain,
    ids,
    route,
    wg,
    wu,
    wd,
    sg,
    gz,
    uz,
    dz,
    bias_rows,
    q_rows,
    mix_rows,
    xr,
    resid,
    dt,
    send_rows,
    recv_rows,
    hx,
    dsend,
    drecv,
    esend,
    erecv,
    back_send,
    back_recv,
    comb_hi,
    comb_lo,
    pick,
    load_sem,
    cache_sem,
    weight_sem,
    z_local_sem,
    z_send,
    z_recv,
    x_send,
    x_recv,
    a_send,
    a_recv,
    t_send,
    t_recv,
    h_send,
    h_recv,
    d_send,
    d_recv,
    e_send,
    e_recv,
    b_send,
    b_recv,
):
    ep = lax.axis_index("ep")
    tp = lax.axis_index("tp")
    rows, width = tok.shape
    n_z = n_ep // GROUP
    g = lax.rem(ep, GROUP)
    base = ep - g
    head = qg.shape[1]
    span = width // n_tp
    units = gz.shape[1]

    def x_peer(k):
        return {"ep": ep, "tp": lax.rem(tp + k, n_tp)}

    def group_peer(k):
        return {"ep": base + lax.rem(g + k, GROUP), "tp": tp}

    def z_peer(k):
        return {"ep": lax.rem(ep + GROUP * k, n_ep), "tp": tp}

    small = [
        (tokens_h, tok),
        (attn_gain_h, again),
        (w_query_h, wq),
        (w_key_h, wk),
        (w_value_h, wv),
        (w_forget_h, wf),
        (forget_bias_h, fb),
        (query_gain_h, qg),
        (key_gain_h, kg),
        (cum_h, cum),
        (lengths_h, lens),
    ]
    loads = [pltpu.make_async_copy(s, d, load_sem.at[i]) for i, (s, d) in enumerate(small)]
    for c in loads:
        c.start()
    barrier = pltpu.get_barrier_semaphore()

    def greet(k, carry):
        pl.semaphore_signal(
            barrier,
            inc=1,
            device_id={"ep": lax.rem(ep + k, n_ep), "tp": tp},
            device_id_type=MESH,
        )
        return carry

    lax.fori_loop(1, n_ep, greet, 0)
    for k in range(1, n_tp):
        pl.semaphore_signal(barrier, inc=1, device_id=x_peer(k), device_id_type=MESH)
    cache_loads = []
    for s in range(rows):
        c = pltpu.make_async_copy(
            cache_h.at[s, 0], cache.at[s // 2, :, pl.ds(128 * (s % 2), 128)], cache_sem.at[s]
        )
        c.start()
        cache_loads.append(c)
    later = [
        (w_output_h, wo),
        (ffn_gain_h, fgain),
        (ids_h, ids),
        (route_h, route),
        (shared_gate_h, sg),
        (w_gate_h.at[0], wg),
        (w_up_h.at[0], wu),
        (w_down_h.at[0], wd),
    ]
    late_loads = [pltpu.make_async_copy(s, d, weight_sem.at[i]) for i, (s, d) in enumerate(later)]
    for c in late_loads:
        c.start()
    quarter = pl.ds(pl.multiple_of(tp * units, units), units)
    own_dense = [
        pltpu.make_async_copy(dense_gate_h.at[quarter], gz.at[0], z_local_sem.at[0]),
        pltpu.make_async_copy(dense_up_h.at[quarter], uz.at[0], z_local_sem.at[1]),
        pltpu.make_async_copy(dense_down_h, dz.at[0], z_local_sem.at[2]),
    ]
    for c in own_dense:
        c.start()

    for c in loads:
        c.wait()
    tokens_f = tok[...].astype(F32)
    normed = (tokens_f * rms(tokens_f) * again[...]).astype(BF)
    query_raw = dot(normed, wq[...])
    key_raw = dot_nt(normed, wk[...])
    value_new = dot_nt(normed, wv[...]).astype(BF)
    forget = jnp.sum(normed.astype(F32) * wf[...].astype(F32), axis=1, keepdims=True)
    forget = forget + fb[...]
    log_gate = jnp.minimum(forget, 0.0) - jnp.log1p(jnp.exp(-jnp.abs(forget)))

    lane_q = iota((rows, span), 1)
    squares = query_raw * query_raw
    scale = jnp.zeros((rows, span), F32)
    for h in range(span // head):
        here = lane_q // head == h
        total = jnp.sum(jnp.where(here, squares, 0.0), axis=1, keepdims=True)
        scale = jnp.where(here, lax.rsqrt(total / head + EPSILON), scale)
    gains = jnp.concatenate([qg[...]] * (span // head), axis=1)
    queries = (query_raw * scale * gains).astype(BF).astype(F32) * head ** (-0.5)
    queries = queries.astype(BF)
    key_new = (key_raw * rms(key_raw) * kg[...]).astype(BF)

    heads = span // head
    n_rows = rows * heads
    row_r = iota((n_rows, 256), 0)
    lane_r = iota((n_rows, 256), 1)
    seq_of = one_hot(iota((n_rows, rows), 0) // heads == iota((n_rows, rows), 1))
    own_half = lane_r // 128 == (row_r // heads) % 2
    own_head = lane_r // head == row_r % heads
    low = own_half & (lane_r % 128 < head)
    high = own_half & (lane_r % 128 >= head)
    fold = one_hot(iota((256, 256), 0) % head == iota((256, 256), 1) % head)
    spread = one_hot(iota((head, 256), 0) == iota((head, 256), 1) % head)

    q_all = jnp.where(own_head, dot(seq_of, queries), 0.0).astype(BF)
    q_wide = jnp.where(low, dot(q_all, fold), 0.0)
    q_rows[...] = q_wide
    key_wide = dot(seq_of, dot(key_new, spread).astype(BF))
    own_score = jnp.sum(q_wide * key_wide, axis=1, keepdims=True)
    value_wide = jnp.where(high, dot(seq_of, dot(value_new, spread).astype(BF)), 0.0)

    cum_2d = cum[...].reshape(rows, cum.shape[2])
    slots = cum_2d.shape[1]
    lens_f = lens[...].astype(F32)
    lens_col = jnp.sum(
        jnp.where(iota((rows, rows), 0) == iota((rows, rows), 1), lens_f, 0.0),
        axis=1,
        keepdims=True,
    )
    position = iota((rows, slots), 1).astype(F32)
    last_cum = jnp.sum(jnp.where(position == lens_col - 1.0, cum_2d, 0.0), axis=1, keepdims=True)
    now_cum = last_cum + log_gate
    bias_rows[...] = jnp.where(position < lens_col, now_cum - cum_2d, NEG)

    pl.semaphore_wait(barrier, n_ep - 1 + n_tp - 1)
    z_copies = []
    for k in (4, 3, 5, 2, 6, 1, 7):
        for i, (src, dst) in enumerate(
            ((dense_gate_h.at[quarter], gz), (dense_up_h.at[quarter], uz), (dense_down_h, dz))
        ):
            z_copies.append(
                pltpu.make_async_remote_copy(
                    src_ref=src,
                    dst_ref=dst.at[k],
                    send_sem=z_send.at[i, k],
                    recv_sem=z_recv.at[i, k],
                    device_id=z_peer(k),
                    device_id_type=MESH,
                )
            )
    for c in z_copies:
        c.start()

    pair = 2 * heads
    first = iota((pair, slots), 0) < heads
    own_probs = []
    for p in range(rows // 2):
        cache_loads[2 * p].wait()
        cache_loads[2 * p + 1].wait()
        q_pair = q_rows[pl.ds(pair * p, pair), :].astype(BF)
        score = jnp.concatenate(
            [dot_nt(q_pair, cache[p, pl.ds(256 * c, 256), :]) for c in range(slots // 256)], axis=1
        )
        decay = jnp.where(
            first,
            jnp.broadcast_to(bias_rows[pl.ds(2 * p, 1), :], (pair, slots)),
            jnp.broadcast_to(bias_rows[pl.ds(2 * p + 1, 1), :], (pair, slots)),
        )
        score = score + decay
        own = own_score[pair * p : pair * (p + 1)]
        peak = jnp.maximum(jnp.max(score, axis=1, keepdims=True), own)
        past = jnp.exp(score - peak)
        own_exp = jnp.exp(own - peak)
        inverse = 1.0 / (jnp.sum(past, axis=1, keepdims=True) + own_exp)
        prob = (past * inverse).astype(BF)
        own_probs.append((own_exp * inverse).astype(BF).astype(F32))
        mix_rows[pl.ds(pair * p, pair), :] = dot(prob, cache[p])
    mixed = jnp.where(high, mix_rows[...], 0.0)
    mixed = mixed + jnp.concatenate(own_probs, axis=0) * value_wide
    by_head = jnp.where(own_head, dot(mixed.astype(BF), fold), 0.0).astype(BF)
    to_seq = one_hot(iota((rows, n_rows), 1) // heads == iota((rows, n_rows), 0))
    head_mix = dot(to_seq, by_head).astype(BF)
    for c in late_loads[:5]:
        c.wait()
    xr[0] = dot(head_mix, wo[...]).astype(BF)
    x_copies = []
    for k in (2, 1, 3):
        c = pltpu.make_async_remote_copy(
            src_ref=xr.at[0],
            dst_ref=xr.at[k],
            send_sem=x_send.at[k],
            recv_sem=x_recv.at[k],
            device_id=x_peer(k),
            device_id_type=MESH,
        )
        c.start()
        x_copies.append(c)

    n_pick = 2 * n_ep
    tokens_all = ids.shape[1]
    window = 256
    first_lane = ep * rows
    start = jnp.minimum(first_lane // 128, (tokens_all - window) // 128) * 128
    offset = first_lane - start
    pick_lanes = iota((window, 128), 0) == iota((window, 128), 1) + offset
    pick_lanes = jnp.where(pick_lanes & (iota((window, 128), 1) < rows), 1.0, 0.0)
    lanes = pl.ds(pl.multiple_of(start, 128), window)
    both = jnp.concatenate([ids[:, lanes].astype(F32), route[:, lanes]], axis=0)
    mine = jnp.dot(both, pick_lanes, precision=lax.Precision.HIGHEST, preferred_element_type=F32)
    lane_p = iota((n_pick, 128), 1)
    expert = (iota((n_pick, 128), 0) // 2).astype(F32)
    live = lane_p < rows
    hit_0 = (mine[0:1] == expert) & live
    hit_1 = (mine[1:2] == expert) & live
    hit = one_hot(hit_0 | hit_1)
    rank = dot(hit, one_hot(iota((128, 128), 0) <= iota((128, 128), 1)))
    slot = (iota((n_pick, 128), 0) % 2 + 1).astype(F32)
    picked = jnp.where((rank == slot) & (hit.astype(F32) > 0.5), 1.0, 0.0)
    pick[...] = picked.astype(BF)
    weight = jnp.where(hit_0, mine[2:3], 0.0) + jnp.where(hit_1, mine[3:4], 0.0)
    combine = (picked * weight).T
    combine_hi = combine.astype(BF)
    comb_hi[...] = combine_hi
    comb_lo[...] = (combine - combine_hi.astype(F32)).astype(BF)

    for c in x_copies:
        c.wait_recv()
    attn_out = xr[0].astype(F32) + xr[1].astype(F32) + xr[2].astype(F32) + xr[3].astype(F32)
    residual = (tok[...].astype(F32) + attn_out).astype(BF).astype(F32)
    resid[...] = residual
    normed_two = (residual * rms(residual) * fgain[...]).astype(BF)
    dt[0] = normed_two
    mix_gate = jnp.sum(normed_two.astype(F32) * sg[...].astype(F32), axis=1, keepdims=True)
    mix_gate = 1.0 / (1.0 + jnp.exp(-mix_gate))
    packed = dot(pick[:, :rows], normed_two).astype(BF)
    send_rows[...] = packed.reshape(n_ep, 2, width)
    recv_rows[ep] = send_rows[ep]

    def dispatch(k, carry):
        to = lax.rem(ep + k, n_ep)
        pltpu.make_async_remote_copy(
            src_ref=send_rows.at[to],
            dst_ref=recv_rows.at[ep],
            send_sem=a_send,
            recv_sem=a_recv,
            device_id={"ep": to, "tp": tp},
            device_id_type=MESH,
        ).start()
        return carry

    lax.fori_loop(1, n_ep, dispatch, 0)
    t_copies = []
    for k in range(1, GROUP):
        c = pltpu.make_async_remote_copy(
            src_ref=dt.at[0],
            dst_ref=dt.at[k],
            send_sem=t_send.at[k],
            recv_sem=t_recv.at[k],
            device_id=group_peer(k),
            device_id_type=MESH,
        )
        c.start()
        t_copies.append(c)

    for c in late_loads[5:]:
        c.wait()
    others = pl.ds(0, n_ep - 1)
    arrivals = pltpu.make_async_remote_copy(
        src_ref=send_rows.at[others],
        dst_ref=recv_rows.at[others],
        send_sem=a_send,
        recv_sem=a_recv,
        device_id=x_peer(1),
        device_id_type=MESH,
    )
    arrivals.wait_recv()
    routed = recv_rows[...].reshape(n_pick, width)
    hidden = (silu(dot(routed, wg[...])) * dot(routed, wu[...])).astype(BF)
    e_copies = []
    for k in (2, 1, 3, 0):
        column = pl.ds(pl.multiple_of(lax.rem(tp + k, n_tp) * span, span), span)
        esend[k] = dot(hidden, wd[:, column]).astype(BF)
        if k:
            c = pltpu.make_async_remote_copy(
                src_ref=esend.at[k],
                dst_ref=erecv.at[k],
                send_sem=e_send.at[k],
                recv_sem=e_recv.at[k],
                device_id=x_peer(k),
                device_id_type=MESH,
            )
            c.start()
            e_copies.append(c)

    for c in own_dense:
        c.wait()
    for c in z_copies:
        c.wait_recv()
    for c in t_copies:
        c.wait_recv()
    group_rows = dt[...].reshape(GROUP * rows, width)
    dense_w = n_z * units
    dense_gate = dot_nt(group_rows, gz[...].reshape(dense_w, width))
    dense_up = dot_nt(group_rows, uz[...].reshape(dense_w, width))
    hx[0] = (silu(dense_gate) * dense_up).astype(BF)
    h_copies = []
    for k in (2, 1, 3):
        c = pltpu.make_async_remote_copy(
            src_ref=hx.at[0],
            dst_ref=hx.at[k],
            send_sem=h_send.at[k],
            recv_sem=h_recv.at[k],
            device_id=x_peer(k),
            device_id_type=MESH,
        )
        c.start()
        h_copies.append(c)

    for c in e_copies:
        c.wait_recv()
    summed = esend[0].astype(F32) + erecv[1].astype(F32) + erecv[2].astype(F32)
    summed = (summed + erecv[3].astype(F32)).astype(BF)
    back_send[...] = summed.reshape(n_ep, 2, span)
    back_recv[ep] = back_send[ep]

    def give_back(k, carry):
        to = lax.rem(ep + k, n_ep)
        pltpu.make_async_remote_copy(
            src_ref=back_send.at[to],
            dst_ref=back_recv.at[ep],
            send_sem=b_send,
            recv_sem=b_recv,
            device_id={"ep": to, "tp": tp},
            device_id_type=MESH,
        ).start()
        return carry

    lax.fori_loop(1, n_ep, give_back, 0)

    for c in h_copies:
        c.wait_recv()
    dense_part = jnp.zeros((GROUP * rows, span), F32)
    for k in range(n_tp):
        owner = lax.rem(tp + n_tp - k, n_tp)
        part = dz[:, pl.ds(pl.multiple_of(owner * units, units), units), :]
        dense_part = dense_part + dot(hx[k], part.reshape(dense_w, span))
    dsend[...] = dense_part.astype(BF).reshape(GROUP, rows, span)
    d_copies = []
    for k in range(1, GROUP):
        c = pltpu.make_async_remote_copy(
            src_ref=dsend.at[k],
            dst_ref=drecv.at[k],
            send_sem=d_send.at[k],
            recv_sem=d_recv.at[k],
            device_id=group_peer(GROUP - k),
            device_id_type=MESH,
        )
        c.start()
        d_copies.append(c)
    for c in d_copies:
        c.wait_recv()
    dense_sum = dsend[0].astype(F32)
    for k in range(1, GROUP):
        dense_sum = dense_sum + drecv[k].astype(F32)

    returned = pltpu.make_async_remote_copy(
        src_ref=back_send.at[others],
        dst_ref=back_recv.at[others],
        send_sem=b_send,
        recv_sem=b_recv,
        device_id=x_peer(1),
        device_id_type=MESH,
    )
    returned.wait_recv()
    expert_rows = back_recv[...].reshape(n_pick, span)
    expert_sum = dot(comb_hi[...], expert_rows) + dot(comb_lo[...], expert_rows)
    mine_cols = pl.ds(pl.multiple_of(tp * span, span), span)
    out = resid[:, mine_cols] + expert_sum[:rows] + mix_gate * dense_sum
    out_ref[...] = out.astype(BF)

    for c in z_copies + x_copies + t_copies + e_copies + h_copies + d_copies:
        c.wait_send()
    arrivals.wait_send()
    returned.wait_send()


def solution(mesh):
    n_ep, n_tp = mesh.shape["ep"], mesh.shape["tp"]

    def shards(*args):
        (
            tokens,
            attn_gain,
            w_query,
            w_key,
            w_value,
            w_forget,
            forget_bias,
            query_gain,
            key_gain,
            cache_pairs,
            cache_cum,
            lengths,
            w_output,
            ffn_gain,
            expert_ids,
            route_weight,
            w_exp_gate,
            w_exp_up,
            w_exp_down,
            shared_gate,
            w_dense_gate,
            w_dense_up,
            w_dense_down,
        ) = args
        rows, width = tokens.shape
        head = query_gain.shape[0]
        slots = cache_pairs.shape[2]
        span = width // n_tp
        n_rows = rows * (w_query.shape[1] // head)
        units = w_dense_gate.shape[0] // n_tp
        n_z = n_ep // GROUP
        ff = w_exp_gate.shape[2]
        n_pick = 2 * n_ep
        operands = (
            tokens,
            attn_gain.reshape(1, -1),
            w_query,
            w_key.T,
            w_value.T,
            w_forget.T,
            forget_bias.reshape(1, -1),
            query_gain.reshape(1, -1),
            key_gain.reshape(1, -1),
            cache_pairs,
            cache_cum,
            lengths.reshape(1, -1),
            w_output,
            ffn_gain.reshape(1, -1),
            expert_ids.T,
            route_weight.T,
            w_exp_gate,
            w_exp_up,
            w_exp_down,
            shared_gate.reshape(1, -1),
            w_dense_gate,
            w_dense_up,
            w_dense_down,
        )
        dma = pltpu.SemaphoreType.DMA
        vmem = pltpu.VMEM
        like = lambda a: vmem(a.shape, a.dtype)
        scratch = [
            like(tokens),
            like(operands[1]),
            like(w_query),
            like(operands[3]),
            like(operands[4]),
            like(operands[5]),
            like(operands[6]),
            like(operands[7]),
            like(operands[8]),
            vmem((rows // 2, slots, 256), BF),
            like(cache_cum),
            like(operands[11]),
            like(w_output),
            like(operands[13]),
            like(operands[14]),
            like(operands[15]),
            vmem((width, ff), BF),
            vmem((width, ff), BF),
            vmem((ff, width), BF),
            like(operands[19]),
            vmem((n_z, units, width), BF),
            vmem((n_z, units, width), BF),
            vmem((n_z, units * n_tp, span), BF),
            vmem((rows, slots), F32),
            vmem((n_rows, 256), F32),
            vmem((n_rows, 256), F32),
            vmem((n_tp, rows, width), BF),
            vmem((rows, width), F32),
            vmem((GROUP, rows, width), BF),
            vmem((n_ep, 2, width), BF),
            vmem((n_ep, 2, width), BF),
            vmem((n_tp, GROUP * rows, n_z * units), BF),
            vmem((GROUP, rows, span), BF),
            vmem((GROUP, rows, span), BF),
            vmem((n_tp, n_pick, span), BF),
            vmem((n_tp, n_pick, span), BF),
            vmem((n_ep, 2, span), BF),
            vmem((n_ep, 2, span), BF),
            vmem((128, n_pick), BF),
            vmem((128, n_pick), BF),
            vmem((n_pick, 128), BF),
            dma((11,)),
            dma((rows,)),
            dma((8,)),
            dma((3,)),
            dma((3, n_z)),
            dma((3, n_z)),
            dma((n_tp,)),
            dma((n_tp,)),
            dma,
            dma,
            dma((GROUP,)),
            dma((GROUP,)),
            dma((n_tp,)),
            dma((n_tp,)),
            dma((GROUP,)),
            dma((GROUP,)),
            dma((n_tp,)),
            dma((n_tp,)),
            dma,
            dma,
        ]
        return pl.pallas_call(
            functools.partial(kernel, n_ep, n_tp),
            out_shape=jax.ShapeDtypeStruct((rows, span), BF),
            in_specs=[pl.BlockSpec(memory_space=pltpu.HBM)] * len(operands),
            out_specs=pl.BlockSpec(memory_space=pltpu.VMEM),
            scratch_shapes=scratch,
            name="layer",
            compiler_params=pltpu.CompilerParams(
                collective_id=0, has_side_effects=True, vmem_limit_bytes=56 * 1024 * 1024
            ),
        )(*operands)

    return jax.shard_map(
        shards,
        mesh=mesh,
        in_specs=(
            P("ep", None),
            P(),
            P(None, "tp"),
            P(None, "tp"),
            P(None, "tp"),
            P(None, "tp"),
            P("tp"),
            P(),
            P(),
            P("ep", "tp", None, None),
            P("ep", "tp", None),
            P("ep"),
            P("tp", None),
            P(),
            P(),
            P(),
            P("ep", None, "tp"),
            P("ep", None, "tp"),
            P("ep", "tp", None),
            P(),
            P("ep", None),
            P("ep", None),
            P("ep", "tp"),
        ),
        out_specs=P("ep", "tp"),
        check_vma=False,
    )
```

```python
import functools

import jax
import jax.numpy as jnp
from jax import lax
from jax.experimental import pallas as pl
from jax.experimental.pallas import tpu as pltpu
from jax.sharding import PartitionSpec as P

EPSILON = 1e-06
MESH = pl.DeviceIdType.MESH
BF = jnp.bfloat16
F32 = jnp.float32
GROUP = 8
NEG = -1e30


def iota(shape, dim):
    return lax.broadcasted_iota(jnp.int32, shape, dim)


def dot(a, b):
    return jnp.dot(a, b, preferred_element_type=F32)


def dot_nt(a, b):
    return lax.dot_general(a, b, (((1,), (1,)), ((), ())), preferred_element_type=F32)


def rms(values):
    return lax.rsqrt(jnp.mean(values * values, axis=-1, keepdims=True) + EPSILON)


def silu(v):
    return v / (1.0 + jnp.exp(-v))


def one_hot(cond):
    return jnp.where(cond, 1.0, 0.0).astype(BF)


def kernel(
    n_ep,
    n_tp,
    tokens_h,
    attn_gain_h,
    w_query_h,
    w_key_h,
    w_value_h,
    w_forget_h,
    forget_bias_h,
    query_gain_h,
    key_gain_h,
    cache_h,
    cum_h,
    lengths_h,
    w_output_h,
    ffn_gain_h,
    ids_h,
    route_h,
    w_gate_h,
    w_up_h,
    w_down_h,
    shared_gate_h,
    dense_gate_h,
    dense_up_h,
    dense_down_h,
    out_ref,
    tok,
    again,
    wq,
    wk,
    wv,
    wf,
    fb,
    qg,
    kg,
    cache,
    cum,
    lens,
    wo,
    fgain,
    ids,
    route,
    wg,
    wu,
    wd,
    sg,
    gz,
    dz,
    bias_rows,
    q_rows,
    mix_rows,
    scores,
    xr,
    resid,
    dt,
    send_rows,
    recv_rows,
    hx,
    dsend,
    drecv,
    esend,
    erecv,
    back_send,
    back_recv,
    comb_hi,
    comb_lo,
    pick,
    load_sem,
    cache_sem,
    weight_sem,
    z_local_sem,
    z_send,
    z_recv,
    x_send,
    x_recv,
    a_send,
    a_recv,
    t_send,
    t_recv,
    h_send,
    h_recv,
    d_send,
    d_recv,
    e_send,
    e_recv,
    b_send,
    b_recv,
):
    ep = lax.axis_index("ep")
    tp = lax.axis_index("tp")
    rows, width = tok.shape
    n_z = n_ep // GROUP
    g = lax.rem(ep, GROUP)
    base = ep - g
    head = qg.shape[1]
    span = width // n_tp
    units = gz.shape[2]

    def x_peer(k):
        return {"ep": ep, "tp": lax.rem(tp + k, n_tp)}

    def group_peer(k):
        return {"ep": base + lax.rem(g + k, GROUP), "tp": tp}

    def z_peer(k):
        return {"ep": lax.rem(ep + GROUP * k, n_ep), "tp": tp}

    small = [
        (tokens_h, tok),
        (attn_gain_h, again),
        (w_query_h, wq),
        (w_key_h, wk),
        (w_value_h, wv),
        (w_forget_h, wf),
        (forget_bias_h, fb),
        (query_gain_h, qg),
        (key_gain_h, kg),
        (cum_h, cum),
        (lengths_h, lens),
    ]
    loads = [pltpu.make_async_copy(s, d, load_sem.at[i]) for i, (s, d) in enumerate(small)]
    for c in loads:
        c.start()
    cache_loads = []
    for s in range(rows):
        c = pltpu.make_async_copy(
            cache_h.at[s, 0], cache.at[s], cache_sem.at[s]
        )
        c.start()
        cache_loads.append(c)
    barrier = pltpu.get_barrier_semaphore()

    def greet(k, carry):
        pl.semaphore_signal(
            barrier,
            inc=1,
            device_id={"ep": lax.rem(ep + k, n_ep), "tp": tp},
            device_id_type=MESH,
        )
        return carry

    lax.fori_loop(1, n_ep, greet, 0)
    for k in range(1, n_tp):
        pl.semaphore_signal(barrier, inc=1, device_id=x_peer(k), device_id_type=MESH)
    later = [
        (w_output_h, wo),
        (ffn_gain_h, fgain),
        (ids_h, ids),
        (route_h, route),
        (shared_gate_h, sg),
        (w_gate_h.at[0], wg),
        (w_up_h.at[0], wu),
        (w_down_h.at[0], wd),
    ]
    late_loads = [pltpu.make_async_copy(s, d, weight_sem.at[i]) for i, (s, d) in enumerate(later)]
    for c in late_loads:
        c.start()
    quarter = pl.ds(pl.multiple_of(tp * units, units), units)
    own_dense = [
        pltpu.make_async_copy(dense_gate_h.at[quarter], gz.at[0, 0], z_local_sem.at[0]),
        pltpu.make_async_copy(dense_up_h.at[quarter], gz.at[0, 1], z_local_sem.at[1]),
        pltpu.make_async_copy(dense_down_h, dz.at[0], z_local_sem.at[2]),
    ]
    for c in own_dense:
        c.start()

    z_copies = {}

    def pass_on(t):
        for come, go, to in ((t, t + 1, 1), ((n_z - t) % n_z, n_z - 1 - t, n_z - 1)):
            if (t < n_z // 2) if to == 1 else (t < n_z - 1 - n_z // 2):
                if t:
                    for c in z_copies[come]:
                        c.wait_recv()
                z_copies[go] = [
                    pltpu.make_async_remote_copy(
                        src_ref=held.at[come],
                        dst_ref=held.at[go],
                        send_sem=z_send.at[i, go],
                        recv_sem=z_recv.at[i, go],
                        device_id=z_peer(to),
                        device_id_type=MESH,
                    )
                    for i, held in enumerate((gz, dz))
                ]
                for c in z_copies[go]:
                    c.start()

    for c in loads:
        c.wait()
    tokens_f = tok[...].astype(F32)
    normed = (tokens_f * rms(tokens_f) * again[...]).astype(BF)
    query_raw = dot(normed, wq[...])
    key_raw = dot_nt(normed, wk[...])
    value_new = dot_nt(normed, wv[...]).astype(BF)
    forget = jnp.sum(normed.astype(F32) * wf[...].astype(F32), axis=1, keepdims=True)
    forget = forget + fb[...]
    log_gate = jnp.minimum(forget, 0.0) - jnp.log1p(jnp.exp(-jnp.abs(forget)))

    lane_q = iota((rows, span), 1)
    squares = query_raw * query_raw
    scale = jnp.zeros((rows, span), F32)
    for h in range(span // head):
        here = lane_q // head == h
        total = jnp.sum(jnp.where(here, squares, 0.0), axis=1, keepdims=True)
        scale = jnp.where(here, lax.rsqrt(total / head + EPSILON), scale)
    gains = jnp.concatenate([qg[...]] * (span // head), axis=1)
    queries = (query_raw * scale * gains).astype(BF).astype(F32) * head ** (-0.5)
    queries = queries.astype(BF)
    key_new = (key_raw * rms(key_raw) * kg[...]).astype(BF)

    heads = span // head
    n_rows = rows * heads
    row_r = iota((n_rows, 256), 0)
    lane_r = iota((n_rows, 256), 1)
    seq_of = one_hot(iota((n_rows, rows), 0) // heads == iota((n_rows, rows), 1))
    own_half = lane_r // 128 == (row_r // heads) % 2
    own_head = lane_r // head == row_r % heads
    low = own_half & (lane_r % 128 < head)
    high = own_half & (lane_r % 128 >= head)
    fold = one_hot(iota((256, 256), 0) % head == iota((256, 256), 1) % head)
    spread = one_hot(iota((head, 256), 0) == iota((head, 256), 1) % head)

    q_all = jnp.where(own_head, dot(seq_of, queries), 0.0).astype(BF)
    q_wide = jnp.where(low, dot(q_all, fold), 0.0)
    q_rows[...] = q_wide
    key_wide = dot(seq_of, dot(key_new, spread).astype(BF))
    own_score = jnp.sum(q_wide * key_wide, axis=1, keepdims=True)
    value_wide = jnp.where(high, dot(seq_of, dot(value_new, spread).astype(BF)), 0.0)

    cum_2d = cum[...].reshape(rows, cum.shape[2])
    slots = cum_2d.shape[1]
    lens_f = lens[...].astype(F32)
    lens_col = jnp.sum(
        jnp.where(iota((rows, rows), 0) == iota((rows, rows), 1), lens_f, 0.0),
        axis=1,
        keepdims=True,
    )
    position = iota((rows, slots), 1).astype(F32)
    last_cum = jnp.sum(jnp.where(position == lens_col - 1.0, cum_2d, 0.0), axis=1, keepdims=True)
    now_cum = last_cum + log_gate
    bias_rows[...] = jnp.where(position < lens_col, now_cum - cum_2d, NEG)

    pair = 2 * heads
    per = 3
    batches = rows // 2 // per
    batch_rows = per * pair

    def both_of(p, c):
        at = pl.ds(256 * c, 256)
        return jnp.concatenate([cache[2 * p, at, :], cache[2 * p + 1, at, :]], axis=1)

    def score_batch(b):
        for i in range(2 * per * b, 2 * per * (b + 1)):
            cache_loads[i].wait()
        for p in range(per * b, per * (b + 1)):
            q_pair = q_rows[pl.ds(pair * p, pair), :].astype(BF)
            for c in range(slots // 256):
                scores[pl.ds(pair * p, pair), pl.ds(256 * c, 256)] = dot_nt(q_pair, both_of(p, c))

    first = iota((pair, slots), 0) < heads
    totals = []
    own_parts = []
    score_batch(0)
    for b in range(batches):
        if b + 1 < batches:
            score_batch(b + 1)
        if b == 1:
            pl.semaphore_wait(barrier, n_ep - 1 + n_tp - 1)
            for c in own_dense:
                c.wait()
            pass_on(0)
        decay = jnp.concatenate(
            [
                jnp.where(
                    first,
                    jnp.broadcast_to(bias_rows[pl.ds(2 * p, 1), :], (pair, slots)),
                    jnp.broadcast_to(bias_rows[pl.ds(2 * p + 1, 1), :], (pair, slots)),
                )
                for p in range(per * b, per * (b + 1))
            ],
            axis=0,
        )
        here = pl.ds(batch_rows * b, batch_rows)
        score = scores[here, :] + decay
        own = own_score[batch_rows * b : batch_rows * (b + 1)]
        peak = jnp.maximum(jnp.max(score, axis=1, keepdims=True), own)
        past = jnp.exp(score - peak)
        own_exp = jnp.exp(own - peak)
        totals.append(jnp.sum(past, axis=1, keepdims=True) + own_exp)
        own_parts.append(own_exp)
        prob = past.astype(BF)
        for i in range(per):
            p = per * b + i
            prob_pair = prob[pair * i : pair * (i + 1)]
            total = dot(prob_pair[:, :256], both_of(p, 0))
            for c in range(1, slots // 256):
                total = total + dot(prob_pair[:, 256 * c : 256 * (c + 1)], both_of(p, c))
            mix_rows[pl.ds(pair * p, pair), :] = total
    inverse = 1.0 / jnp.concatenate(totals, axis=0)
    mixed = jnp.where(high, mix_rows[...], 0.0)
    mixed = (mixed + jnp.concatenate(own_parts, axis=0) * value_wide) * inverse
    by_head = jnp.where(own_head, dot(mixed.astype(BF), fold), 0.0).astype(BF)
    to_seq = one_hot(iota((rows, n_rows), 1) // heads == iota((rows, n_rows), 0))
    head_mix = dot(to_seq, by_head).astype(BF)
    for c in late_loads[:5]:
        c.wait()
    xr[0] = dot(head_mix, wo[...]).astype(BF)
    x_copies = []
    for k in (2, 1, 3):
        c = pltpu.make_async_remote_copy(
            src_ref=xr.at[0],
            dst_ref=xr.at[k],
            send_sem=x_send.at[k],
            recv_sem=x_recv.at[k],
            device_id=x_peer(k),
            device_id_type=MESH,
        )
        c.start()
        x_copies.append(c)

    pass_on(1)

    n_pick = 2 * n_ep
    tokens_all = ids.shape[1]
    window = 256
    first_lane = ep * rows
    start = jnp.minimum(first_lane // 128, (tokens_all - window) // 128) * 128
    offset = first_lane - start
    pick_lanes = iota((window, 128), 0) == iota((window, 128), 1) + offset
    pick_lanes = jnp.where(pick_lanes & (iota((window, 128), 1) < rows), 1.0, 0.0)
    lanes = pl.ds(pl.multiple_of(start, 128), window)
    both = jnp.concatenate([ids[:, lanes].astype(F32), route[:, lanes]], axis=0)
    mine = jnp.dot(both, pick_lanes, precision=lax.Precision.HIGHEST, preferred_element_type=F32)
    lane_p = iota((n_pick, 128), 1)
    expert = (iota((n_pick, 128), 0) // 2).astype(F32)
    live = lane_p < rows
    hit_0 = (mine[0:1] == expert) & live
    hit_1 = (mine[1:2] == expert) & live
    hit = one_hot(hit_0 | hit_1)
    rank = dot(hit, one_hot(iota((128, 128), 0) <= iota((128, 128), 1)))
    slot = (iota((n_pick, 128), 0) % 2 + 1).astype(F32)
    picked = jnp.where((rank == slot) & (hit.astype(F32) > 0.5), 1.0, 0.0)
    pick[...] = picked.astype(BF)
    weight = jnp.where(hit_0, mine[2:3], 0.0) + jnp.where(hit_1, mine[3:4], 0.0)
    combine = (picked * weight).T
    combine_hi = combine.astype(BF)
    comb_hi[...] = combine_hi
    comb_lo[...] = (combine - combine_hi.astype(F32)).astype(BF)

    for c in x_copies:
        c.wait_recv()
    attn_out = xr[0].astype(F32) + xr[1].astype(F32) + xr[2].astype(F32) + xr[3].astype(F32)
    residual = (tok[...].astype(F32) + attn_out).astype(BF).astype(F32)
    resid[...] = residual
    normed_two = (residual * rms(residual) * fgain[...]).astype(BF)
    dt[0] = normed_two
    gate_row = sg[...].astype(F32)
    gate_row = jnp.concatenate([gate_row[i : i + 1] for i in range(width // 128)], axis=1)
    mix_gate = jnp.sum(normed_two.astype(F32) * gate_row, axis=1, keepdims=True)
    mix_gate = 1.0 / (1.0 + jnp.exp(-mix_gate))
    packed = dot(pick[:, :rows], normed_two).astype(BF)
    send_rows[...] = packed.reshape(n_ep, 2, width)
    recv_rows[ep] = send_rows[ep]

    def dispatch(k, carry):
        to = lax.rem(ep + k, n_ep)
        pltpu.make_async_remote_copy(
            src_ref=send_rows.at[to],
            dst_ref=recv_rows.at[ep],
            send_sem=a_send,
            recv_sem=a_recv,
            device_id={"ep": to, "tp": tp},
            device_id_type=MESH,
        ).start()
        return carry

    lax.fori_loop(1, n_ep, dispatch, 0)
    t_copies = []
    for k in range(1, GROUP):
        c = pltpu.make_async_remote_copy(
            src_ref=dt.at[0],
            dst_ref=dt.at[k],
            send_sem=t_send.at[k],
            recv_sem=t_recv.at[k],
            device_id=group_peer(k),
            device_id_type=MESH,
        )
        c.start()
        t_copies.append(c)

    pass_on(2)
    pass_on(3)

    for c in late_loads[5:]:
        c.wait()
    others = pl.ds(0, n_ep - 1)
    arrivals = pltpu.make_async_remote_copy(
        src_ref=send_rows.at[others],
        dst_ref=recv_rows.at[others],
        send_sem=a_send,
        recv_sem=a_recv,
        device_id=x_peer(1),
        device_id_type=MESH,
    )
    arrivals.wait_recv()
    routed = recv_rows[...].reshape(n_pick, width)
    hidden = (silu(dot(routed, wg[...])) * dot(routed, wu[...])).astype(BF)
    e_copies = []
    for k in (2, 1, 3, 0):
        column = pl.ds(pl.multiple_of(lax.rem(tp + k, n_tp) * span, span), span)
        esend[k] = dot(hidden, wd[:, column]).astype(BF)
        if k:
            c = pltpu.make_async_remote_copy(
                src_ref=esend.at[k],
                dst_ref=erecv.at[k],
                send_sem=e_send.at[k],
                recv_sem=e_recv.at[k],
                device_id=x_peer(k),
                device_id_type=MESH,
            )
            c.start()
            e_copies.append(c)

    for come in (n_z // 2, n_z - (n_z - 1 - n_z // 2)):
        for c in z_copies[come]:
            c.wait_recv()
    for c in t_copies:
        c.wait_recv()
    group_rows = dt[...].reshape(GROUP * rows, width)
    dense_w = n_z * units
    dense_gate = dot_nt(group_rows, gz[:, 0].reshape(dense_w, width))
    dense_up = dot_nt(group_rows, gz[:, 1].reshape(dense_w, width))
    hx[0] = (silu(dense_gate) * dense_up).astype(BF)
    h_copies = []
    for k in (2, 1, 3):
        c = pltpu.make_async_remote_copy(
            src_ref=hx.at[0],
            dst_ref=hx.at[k],
            send_sem=h_send.at[k],
            recv_sem=h_recv.at[k],
            device_id=x_peer(k),
            device_id_type=MESH,
        )
        c.start()
        h_copies.append(c)

    for c in e_copies:
        c.wait_recv()
    summed = esend[0].astype(F32) + erecv[1].astype(F32) + erecv[2].astype(F32)
    summed = (summed + erecv[3].astype(F32)).astype(BF)
    back_send[...] = summed.reshape(n_ep, 2, span)
    back_recv[ep] = back_send[ep]

    def give_back(k, carry):
        to = lax.rem(ep + k, n_ep)
        pltpu.make_async_remote_copy(
            src_ref=back_send.at[to],
            dst_ref=back_recv.at[ep],
            send_sem=b_send,
            recv_sem=b_recv,
            device_id={"ep": to, "tp": tp},
            device_id_type=MESH,
        ).start()
        return carry

    lax.fori_loop(1, n_ep, give_back, 0)

    for c in h_copies:
        c.wait_recv()
    dense_part = jnp.zeros((GROUP * rows, span), F32)
    for k in range(n_tp):
        owner = lax.rem(tp + n_tp - k, n_tp)
        part = dz[:, pl.ds(pl.multiple_of(owner * units, units), units), :]
        dense_part = dense_part + dot(hx[k], part.reshape(dense_w, span))
    dsend[...] = dense_part.astype(BF).reshape(GROUP, rows, span)
    d_copies = []
    for k in range(1, GROUP):
        c = pltpu.make_async_remote_copy(
            src_ref=dsend.at[k],
            dst_ref=drecv.at[k],
            send_sem=d_send.at[k],
            recv_sem=d_recv.at[k],
            device_id=group_peer(GROUP - k),
            device_id_type=MESH,
        )
        c.start()
        d_copies.append(c)
    for c in d_copies:
        c.wait_recv()
    dense_sum = dsend[0].astype(F32)
    for k in range(1, GROUP):
        dense_sum = dense_sum + drecv[k].astype(F32)

    returned = pltpu.make_async_remote_copy(
        src_ref=back_send.at[others],
        dst_ref=back_recv.at[others],
        send_sem=b_send,
        recv_sem=b_recv,
        device_id=x_peer(1),
        device_id_type=MESH,
    )
    returned.wait_recv()
    expert_rows = back_recv[...].reshape(n_pick, span)
    expert_sum = dot(comb_hi[...], expert_rows) + dot(comb_lo[...], expert_rows)
    mine_cols = pl.ds(pl.multiple_of(tp * span, span), span)
    out = resid[:, mine_cols] + expert_sum[:rows] + mix_gate * dense_sum
    out_ref[...] = out.astype(BF)

    for c in sum(z_copies.values(), []) + x_copies + t_copies + e_copies + h_copies + d_copies:
        c.wait_send()
    arrivals.wait_send()
    returned.wait_send()


def solution(mesh):
    n_ep, n_tp = mesh.shape["ep"], mesh.shape["tp"]

    def shards(*args):
        (
            tokens,
            attn_gain,
            w_query,
            w_key,
            w_value,
            w_forget,
            forget_bias,
            query_gain,
            key_gain,
            cache_pairs,
            cache_cum,
            lengths,
            w_output,
            ffn_gain,
            expert_ids,
            route_weight,
            w_exp_gate,
            w_exp_up,
            w_exp_down,
            shared_gate,
            w_dense_gate,
            w_dense_up,
            w_dense_down,
        ) = args
        rows, width = tokens.shape
        head = query_gain.shape[0]
        slots = cache_pairs.shape[2]
        span = width // n_tp
        n_rows = rows * (w_query.shape[1] // head)
        units = w_dense_gate.shape[0] // n_tp
        n_z = n_ep // GROUP
        ff = w_exp_gate.shape[2]
        n_pick = 2 * n_ep
        operands = (
            tokens,
            attn_gain.reshape(1, -1),
            w_query,
            w_key.T,
            w_value.T,
            w_forget.T,
            forget_bias.reshape(1, -1),
            query_gain.reshape(1, -1),
            key_gain.reshape(1, -1),
            cache_pairs,
            cache_cum,
            lengths.reshape(1, -1),
            w_output,
            ffn_gain.reshape(1, -1),
            expert_ids.T,
            route_weight.T,
            w_exp_gate,
            w_exp_up,
            w_exp_down,
            shared_gate.reshape(-1, 128),
            w_dense_gate,
            w_dense_up,
            w_dense_down,
        )
        dma = pltpu.SemaphoreType.DMA
        vmem = pltpu.VMEM
        like = lambda a: vmem(a.shape, a.dtype)
        scratch = [
            like(tokens),
            like(operands[1]),
            like(w_query),
            like(operands[3]),
            like(operands[4]),
            like(operands[5]),
            like(operands[6]),
            like(operands[7]),
            like(operands[8]),
            vmem((rows, slots, 128), BF),
            like(cache_cum),
            like(operands[11]),
            like(w_output),
            like(operands[13]),
            like(operands[14]),
            like(operands[15]),
            vmem((width, ff), BF),
            vmem((width, ff), BF),
            vmem((ff, width), BF),
            like(operands[19]),
            vmem((n_z, 2, units, width), BF),
            vmem((n_z, units * n_tp, span), BF),
            vmem((rows, slots), F32),
            vmem((n_rows, 256), F32),
            vmem((n_rows, 256), F32),
            vmem((n_rows, slots), F32),
            vmem((n_tp, rows, width), BF),
            vmem((rows, width), F32),
            vmem((GROUP, rows, width), BF),
            vmem((n_ep, 2, width), BF),
            vmem((n_ep, 2, width), BF),
            vmem((n_tp, GROUP * rows, n_z * units), BF),
            vmem((GROUP, rows, span), BF),
            vmem((GROUP, rows, span), BF),
            vmem((n_tp, n_pick, span), BF),
            vmem((n_tp, n_pick, span), BF),
            vmem((n_ep, 2, span), BF),
            vmem((n_ep, 2, span), BF),
            vmem((128, n_pick), BF),
            vmem((128, n_pick), BF),
            vmem((n_pick, 128), BF),
            dma((11,)),
            dma((rows,)),
            dma((8,)),
            dma((3,)),
            dma((2, n_z)),
            dma((2, n_z)),
            dma((n_tp,)),
            dma((n_tp,)),
            dma,
            dma,
            dma((GROUP,)),
            dma((GROUP,)),
            dma((n_tp,)),
            dma((n_tp,)),
            dma((GROUP,)),
            dma((GROUP,)),
            dma((n_tp,)),
            dma((n_tp,)),
            dma,
            dma,
        ]
        return pl.pallas_call(
            functools.partial(kernel, n_ep, n_tp),
            out_shape=jax.ShapeDtypeStruct((rows, span), BF),
            in_specs=[pl.BlockSpec(memory_space=pltpu.HBM)] * len(operands),
            out_specs=pl.BlockSpec(memory_space=pltpu.VMEM),
            scratch_shapes=scratch,
            name="layer",
            compiler_params=pltpu.CompilerParams(
                collective_id=0, has_side_effects=True, vmem_limit_bytes=56 * 1024 * 1024
            ),
        )(*operands)

    return jax.shard_map(
        shards,
        mesh=mesh,
        in_specs=(
            P("ep", None),
            P(),
            P(None, "tp"),
            P(None, "tp"),
            P(None, "tp"),
            P(None, "tp"),
            P("tp"),
            P(),
            P(),
            P("ep", "tp", None, None),
            P("ep", "tp", None),
            P("ep"),
            P("tp", None),
            P(),
            P(),
            P(),
            P("ep", None, "tp"),
            P("ep", None, "tp"),
            P("ep", "tp", None),
            P(),
            P("ep", None),
            P("ep", None),
            P("ep", "tp"),
        ),
        out_specs=P("ep", "tp"),
        check_vma=False,
    )
```

```python
import functools

import jax
import jax.numpy as jnp
from jax import lax
from jax.experimental import pallas as pl
from jax.experimental.pallas import tpu as pltpu
from jax.sharding import PartitionSpec as P

EPSILON = 1e-06
MESH = pl.DeviceIdType.MESH
BF = jnp.bfloat16
F32 = jnp.float32
GROUP = 8
NEG = -1e30


def iota(shape, dim):
    return lax.broadcasted_iota(jnp.int32, shape, dim)


def dot(a, b):
    return jnp.dot(a, b, preferred_element_type=F32)


def dot_nt(a, b):
    return lax.dot_general(a, b, (((1,), (1,)), ((), ())), preferred_element_type=F32)


def rms(values):
    return lax.rsqrt(jnp.mean(values * values, axis=-1, keepdims=True) + EPSILON)


def silu(v):
    return v / (1.0 + jnp.exp(-v))


def one_hot(cond):
    return jnp.where(cond, 1.0, 0.0).astype(BF)


def kernel(
    n_ep,
    n_tp,
    tokens_h,
    attn_gain_h,
    w_query_h,
    w_key_h,
    w_value_h,
    w_forget_h,
    forget_bias_h,
    query_gain_h,
    key_gain_h,
    cache_h,
    cum_h,
    lengths_h,
    w_output_h,
    ffn_gain_h,
    ids_h,
    route_h,
    w_gate_h,
    w_up_h,
    w_down_h,
    shared_gate_h,
    dense_gate_h,
    dense_up_h,
    dense_down_h,
    out_ref,
    tok,
    again,
    wq,
    wk,
    wv,
    wf,
    fb,
    qg,
    kg,
    cache,
    cum,
    lens,
    wo,
    fgain,
    ids,
    route,
    wg,
    wu,
    wd,
    sg,
    gz,
    dz,
    bias_rows,
    q_rows,
    mix_rows,
    scores,
    xr,
    resid,
    dt,
    send_rows,
    recv_rows,
    hx,
    dsend,
    drecv,
    esend,
    erecv,
    back_send,
    back_recv,
    comb_hi,
    comb_lo,
    pick,
    load_sem,
    cache_sem,
    weight_sem,
    z_local_sem,
    z_send,
    z_recv,
    x_send,
    x_recv,
    a_send,
    a_recv,
    t_send,
    t_recv,
    h_send,
    h_recv,
    d_send,
    d_recv,
    e_send,
    e_recv,
    b_send,
    b_recv,
):
    ep = lax.axis_index("ep")
    tp = lax.axis_index("tp")
    rows, width = tok.shape
    n_z = n_ep // GROUP
    g = lax.rem(ep, GROUP)
    base = ep - g
    head = qg.shape[1]
    span = width // n_tp
    units = gz.shape[2]

    z = ep // GROUP
    far_first = [n_z // 2]
    for k in range(1, n_z // 2):
        far_first += [n_z // 2 - k, n_z // 2 + k]
    far_first += [0]
    parts = 2
    part_z = n_z // parts
    part_slots = n_ep // parts

    def ep_peer(far, low):
        return lax.rem(z + far, n_z) * GROUP + lax.rem(g + low, GROUP)

    def exchange(half, source, target, send_sem, recv_sem, back):
        for i in range(part_z * half, part_z * (half + 1)):
            far = far_first[i]

            def one(low, carry):
                if back:
                    to = ep_peer(n_z - far, GROUP - low)
                else:
                    to = ep_peer(far, low)
                pltpu.make_async_remote_copy(
                    src_ref=source.at[GROUP * i + low],
                    dst_ref=target.at[GROUP * i + low],
                    send_sem=send_sem,
                    recv_sem=recv_sem,
                    device_id={"ep": to, "tp": tp},
                    device_id_type=MESH,
                ).start()
                return carry

            lax.fori_loop(0 if far else 1, GROUP, one, 0)

    own_slot = n_ep - GROUP

    def x_peer(k):
        return {"ep": ep, "tp": lax.rem(tp + k, n_tp)}

    def group_peer(k):
        return {"ep": base + lax.rem(g + k, GROUP), "tp": tp}

    def z_peer(k):
        return {"ep": lax.rem(ep + GROUP * k, n_ep), "tp": tp}

    small = [
        (tokens_h, tok),
        (attn_gain_h, again),
        (w_query_h, wq),
        (w_key_h, wk),
        (w_value_h, wv),
        (w_forget_h, wf),
        (forget_bias_h, fb),
        (query_gain_h, qg),
        (key_gain_h, kg),
        (cum_h, cum),
        (lengths_h, lens),
    ]
    loads = [pltpu.make_async_copy(s, d, load_sem.at[i]) for i, (s, d) in enumerate(small)]
    for c in loads:
        c.start()
    cache_loads = []
    for s in range(rows):
        c = pltpu.make_async_copy(
            cache_h.at[s, 0], cache.at[s], cache_sem.at[s]
        )
        c.start()
        cache_loads.append(c)
    barrier = pltpu.get_barrier_semaphore()

    def greet(k, carry):
        pl.semaphore_signal(
            barrier,
            inc=1,
            device_id={"ep": lax.rem(ep + k, n_ep), "tp": tp},
            device_id_type=MESH,
        )
        return carry

    lax.fori_loop(1, n_ep, greet, 0)
    for k in range(1, n_tp):
        pl.semaphore_signal(barrier, inc=1, device_id=x_peer(k), device_id_type=MESH)
    later = [
        (w_output_h, wo),
        (ffn_gain_h, fgain),
        (ids_h, ids),
        (route_h, route),
        (shared_gate_h, sg),
        (w_gate_h.at[0], wg),
        (w_up_h.at[0], wu),
        (w_down_h.at[0], wd),
    ]
    late_loads = [pltpu.make_async_copy(s, d, weight_sem.at[i]) for i, (s, d) in enumerate(later)]
    for c in late_loads[:5]:
        c.start()
    quarter = pl.ds(pl.multiple_of(tp * units, units), units)
    own_dense = [
        pltpu.make_async_copy(dense_gate_h.at[quarter], gz.at[0, 0], z_local_sem.at[0]),
        pltpu.make_async_copy(dense_up_h.at[quarter], gz.at[0, 1], z_local_sem.at[1]),
        pltpu.make_async_copy(dense_down_h, dz.at[0], z_local_sem.at[2]),
    ]
    for c in own_dense:
        c.start()

    z_copies = {}

    def pass_on(t):
        for come, go, to in ((t, t + 1, 1), ((n_z - t) % n_z, n_z - 1 - t, n_z - 1)):
            if (t < n_z // 2) if to == 1 else (t < n_z - 1 - n_z // 2):
                if t:
                    for c in z_copies[come]:
                        c.wait_recv()
                z_copies[go] = [
                    pltpu.make_async_remote_copy(
                        src_ref=held.at[come],
                        dst_ref=held.at[go],
                        send_sem=z_send.at[i, go],
                        recv_sem=z_recv.at[i, go],
                        device_id=z_peer(to),
                        device_id_type=MESH,
                    )
                    for i, held in enumerate((gz, dz))
                ]
                for c in z_copies[go]:
                    c.start()

    for c in loads:
        c.wait()
    tokens_f = tok[...].astype(F32)
    normed = (tokens_f * rms(tokens_f) * again[...]).astype(BF)
    query_raw = dot(normed, wq[...])
    key_raw = dot_nt(normed, wk[...])
    value_new = dot_nt(normed, wv[...]).astype(BF)
    forget = jnp.sum(normed.astype(F32) * wf[...].astype(F32), axis=1, keepdims=True)
    forget = forget + fb[...]
    log_gate = jnp.minimum(forget, 0.0) - jnp.log1p(jnp.exp(-jnp.abs(forget)))

    lane_q = iota((rows, span), 1)
    squares = query_raw * query_raw
    scale = jnp.zeros((rows, span), F32)
    for h in range(span // head):
        here = lane_q // head == h
        total = jnp.sum(jnp.where(here, squares, 0.0), axis=1, keepdims=True)
        scale = jnp.where(here, lax.rsqrt(total / head + EPSILON), scale)
    gains = jnp.concatenate([qg[...]] * (span // head), axis=1)
    queries = (query_raw * scale * gains).astype(BF).astype(F32) * head ** (-0.5)
    queries = queries.astype(BF)
    key_new = (key_raw * rms(key_raw) * kg[...]).astype(BF)

    heads = span // head
    n_rows = rows * heads
    row_r = iota((n_rows, 256), 0)
    lane_r = iota((n_rows, 256), 1)
    seq_of = one_hot(iota((n_rows, rows), 0) // heads == iota((n_rows, rows), 1))
    own_half = lane_r // 128 == (row_r // heads) % 2
    own_head = lane_r // head == row_r % heads
    low = own_half & (lane_r % 128 < head)
    high = own_half & (lane_r % 128 >= head)
    fold = one_hot(iota((256, 256), 0) % head == iota((256, 256), 1) % head)
    spread = one_hot(iota((head, 256), 0) == iota((head, 256), 1) % head)

    q_all = jnp.where(own_head, dot(seq_of, queries), 0.0).astype(BF)
    q_wide = jnp.where(low, dot(q_all, fold), 0.0)
    q_rows[...] = q_wide
    key_wide = dot(seq_of, dot(key_new, spread).astype(BF))
    own_score = jnp.sum(q_wide * key_wide, axis=1, keepdims=True)
    value_wide = jnp.where(high, dot(seq_of, dot(value_new, spread).astype(BF)), 0.0)

    cum_2d = cum[...].reshape(rows, cum.shape[2])
    slots = cum_2d.shape[1]
    lens_f = lens[...].astype(F32)
    lens_col = jnp.sum(
        jnp.where(iota((rows, rows), 0) == iota((rows, rows), 1), lens_f, 0.0),
        axis=1,
        keepdims=True,
    )
    position = iota((rows, slots), 1).astype(F32)
    last_cum = jnp.sum(jnp.where(position == lens_col - 1.0, cum_2d, 0.0), axis=1, keepdims=True)
    now_cum = last_cum + log_gate
    bias_rows[...] = jnp.where(position < lens_col, now_cum - cum_2d, NEG)

    pair = 2 * heads
    per = 3
    batches = rows // 2 // per
    batch_rows = per * pair

    def both_of(p, c):
        at = pl.ds(256 * c, 256)
        return jnp.concatenate([cache[2 * p, at, :], cache[2 * p + 1, at, :]], axis=1)

    def score_batch(b):
        for i in range(2 * per * b, 2 * per * (b + 1)):
            cache_loads[i].wait()
        for p in range(per * b, per * (b + 1)):
            q_pair = q_rows[pl.ds(pair * p, pair), :].astype(BF)
            for c in range(slots // 256):
                scores[pl.ds(pair * p, pair), pl.ds(256 * c, 256)] = dot_nt(q_pair, both_of(p, c))

    first = iota((pair, slots), 0) < heads
    totals = []
    own_parts = []
    score_batch(0)
    for b in range(batches):
        if b + 1 < batches:
            score_batch(b + 1)
        if b == 1:
            for c in late_loads[5:]:
                c.start()
            pl.semaphore_wait(barrier, n_ep - 1 + n_tp - 1)
            for c in own_dense:
                c.wait()
            pass_on(0)
        decay = jnp.concatenate(
            [
                jnp.where(
                    first,
                    jnp.broadcast_to(bias_rows[pl.ds(2 * p, 1), :], (pair, slots)),
                    jnp.broadcast_to(bias_rows[pl.ds(2 * p + 1, 1), :], (pair, slots)),
                )
                for p in range(per * b, per * (b + 1))
            ],
            axis=0,
        )
        here = pl.ds(batch_rows * b, batch_rows)
        score = scores[here, :] + decay
        own = own_score[batch_rows * b : batch_rows * (b + 1)]
        peak = jnp.maximum(jnp.max(score, axis=1, keepdims=True), own)
        past = jnp.exp(score - peak)
        own_exp = jnp.exp(own - peak)
        totals.append(jnp.sum(past, axis=1, keepdims=True) + own_exp)
        own_parts.append(own_exp)
        prob = past.astype(BF)
        for i in range(per):
            p = per * b + i
            prob_pair = prob[pair * i : pair * (i + 1)]
            total = dot(prob_pair[:, :256], both_of(p, 0))
            for c in range(1, slots // 256):
                total = total + dot(prob_pair[:, 256 * c : 256 * (c + 1)], both_of(p, c))
            mix_rows[pl.ds(pair * p, pair), :] = total
    inverse = 1.0 / jnp.concatenate(totals, axis=0)
    mixed = jnp.where(high, mix_rows[...], 0.0)
    mixed = (mixed + jnp.concatenate(own_parts, axis=0) * value_wide) * inverse
    by_head = jnp.where(own_head, dot(mixed.astype(BF), fold), 0.0).astype(BF)
    to_seq = one_hot(iota((rows, n_rows), 1) // heads == iota((rows, n_rows), 0))
    head_mix = dot(to_seq, by_head).astype(BF)
    for c in late_loads[:5]:
        c.wait()
    xr[0] = dot(head_mix, wo[...]).astype(BF)
    x_copies = []
    for k in (2, 1, 3):
        c = pltpu.make_async_remote_copy(
            src_ref=xr.at[0],
            dst_ref=xr.at[k],
            send_sem=x_send.at[k],
            recv_sem=x_recv.at[k],
            device_id=x_peer(k),
            device_id_type=MESH,
        )
        c.start()
        x_copies.append(c)

    pass_on(1)

    n_pick = 2 * n_ep
    tokens_all = ids.shape[1]
    window = 256
    first_lane = ep * rows
    start = jnp.minimum(first_lane // 128, (tokens_all - window) // 128) * 128
    offset = first_lane - start
    pick_lanes = iota((window, 128), 0) == iota((window, 128), 1) + offset
    pick_lanes = jnp.where(pick_lanes & (iota((window, 128), 1) < rows), 1.0, 0.0)
    lanes = pl.ds(pl.multiple_of(start, 128), window)
    both = jnp.concatenate([ids[:, lanes].astype(F32), route[:, lanes]], axis=0)
    mine = jnp.dot(both, pick_lanes, precision=lax.Precision.HIGHEST, preferred_element_type=F32)
    lane_p = iota((n_pick, 128), 1)
    slot_of = iota((n_pick, 128), 0) // 2
    far_of = jnp.zeros((n_pick, 128), jnp.int32)
    for i, far in enumerate(far_first):
        far_of = jnp.where(slot_of // GROUP == i, far, far_of)
    expert = lax.rem(z + far_of, n_z) * GROUP + lax.rem(g + slot_of % GROUP, GROUP)
    expert = expert.astype(F32)
    live = lane_p < rows
    hit_0 = (mine[0:1] == expert) & live
    hit_1 = (mine[1:2] == expert) & live
    hit = one_hot(hit_0 | hit_1)
    rank = dot(hit, one_hot(iota((128, 128), 0) <= iota((128, 128), 1)))
    slot = (iota((n_pick, 128), 0) % 2 + 1).astype(F32)
    picked = jnp.where((rank == slot) & (hit.astype(F32) > 0.5), 1.0, 0.0)
    pick[...] = picked.astype(BF)
    weight = jnp.where(hit_0, mine[2:3], 0.0) + jnp.where(hit_1, mine[3:4], 0.0)
    combine = (picked * weight).T
    combine_hi = combine.astype(BF)
    comb_hi[...] = combine_hi
    comb_lo[...] = (combine - combine_hi.astype(F32)).astype(BF)

    for c in x_copies:
        c.wait_recv()
    attn_out = xr[0].astype(F32) + xr[1].astype(F32) + xr[2].astype(F32) + xr[3].astype(F32)
    residual = (tok[...].astype(F32) + attn_out).astype(BF).astype(F32)
    resid[...] = residual
    normed_two = (residual * rms(residual) * fgain[...]).astype(BF)
    dt[0] = normed_two
    gate_row = sg[...].astype(F32)
    gate_row = jnp.concatenate([gate_row[i : i + 1] for i in range(width // 128)], axis=1)
    mix_gate = jnp.sum(normed_two.astype(F32) * gate_row, axis=1, keepdims=True)
    mix_gate = 1.0 / (1.0 + jnp.exp(-mix_gate))
    for half in range(parts):
        at = pl.ds(2 * part_slots * half, 2 * part_slots)
        packed = dot(pick[at, :rows], normed_two).astype(BF)
        send_rows[pl.ds(part_slots * half, part_slots)] = packed.reshape(part_slots, 2, width)
        exchange(half, send_rows, recv_rows, a_send, a_recv, False)
    recv_rows[own_slot] = send_rows[own_slot]
    t_copies = []
    for k in range(1, GROUP):
        c = pltpu.make_async_remote_copy(
            src_ref=dt.at[0],
            dst_ref=dt.at[k],
            send_sem=t_send.at[k],
            recv_sem=t_recv.at[k],
            device_id=group_peer(k),
            device_id_type=MESH,
        )
        c.start()
        t_copies.append(c)

    pass_on(2)
    pass_on(3)

    for c in late_loads[5:]:
        c.wait()
    others = pl.ds(0, n_ep - 1)
    arrivals = pltpu.make_async_remote_copy(
        src_ref=send_rows.at[others],
        dst_ref=recv_rows.at[others],
        send_sem=a_send,
        recv_sem=a_recv,
        device_id=x_peer(1),
        device_id_type=MESH,
    )
    arrivals.wait_recv()
    routed = recv_rows[...].reshape(n_pick, width)
    hidden = (silu(dot(routed, wg[...])) * dot(routed, wu[...])).astype(BF)
    e_copies = [[], []]
    for k in (2, 1, 3, 0):
        column = pl.ds(pl.multiple_of(lax.rem(tp + k, n_tp) * span, span), span)
        part = dot(hidden, wd[:, column]).astype(BF)
        esend[k] = part.reshape(parts, n_pick // parts, span)
        if k:
            for half in range(parts):
                c = pltpu.make_async_remote_copy(
                    src_ref=esend.at[k, half],
                    dst_ref=erecv.at[k, half],
                    send_sem=e_send.at[k, half],
                    recv_sem=e_recv.at[k, half],
                    device_id=x_peer(k),
                    device_id_type=MESH,
                )
                e_copies[half].append(c)
            e_copies[0][-1].start()
    for c in e_copies[1]:
        c.start()

    for come in (n_z // 2, n_z - (n_z - 1 - n_z // 2)):
        for c in z_copies[come]:
            c.wait_recv()
    for c in t_copies:
        c.wait_recv()
    group_rows = dt[...].reshape(GROUP * rows, width)
    dense_w = n_z * units
    dense_gate = dot_nt(group_rows, gz[:, 0].reshape(dense_w, width))
    dense_up = dot_nt(group_rows, gz[:, 1].reshape(dense_w, width))
    hx[0] = (silu(dense_gate) * dense_up).astype(BF)
    h_copies = []
    for k in (2, 1, 3):
        c = pltpu.make_async_remote_copy(
            src_ref=hx.at[0],
            dst_ref=hx.at[k],
            send_sem=h_send.at[k],
            recv_sem=h_recv.at[k],
            device_id=x_peer(k),
            device_id_type=MESH,
        )
        c.start()
        h_copies.append(c)

    for half in range(parts):
        for c in e_copies[half]:
            c.wait_recv()
        summed = esend[0, half].astype(F32) + erecv[1, half].astype(F32)
        summed = summed + erecv[2, half].astype(F32) + erecv[3, half].astype(F32)
        at = pl.ds(part_slots * half, part_slots)
        back_send[at] = summed.astype(BF).reshape(part_slots, 2, span)
        exchange(half, back_send, back_recv, b_send, b_recv, True)
    back_recv[own_slot] = back_send[own_slot]

    for c in h_copies:
        c.wait_recv()
    dense_part = jnp.zeros((GROUP * rows, span), F32)
    for k in range(n_tp):
        owner = lax.rem(tp + n_tp - k, n_tp)
        part = dz[:, pl.ds(pl.multiple_of(owner * units, units), units), :]
        dense_part = dense_part + dot(hx[k], part.reshape(dense_w, span))
    dsend[...] = dense_part.astype(BF).reshape(GROUP, rows, span)
    d_copies = []
    for k in range(1, GROUP):
        c = pltpu.make_async_remote_copy(
            src_ref=dsend.at[k],
            dst_ref=drecv.at[k],
            send_sem=d_send.at[k],
            recv_sem=d_recv.at[k],
            device_id=group_peer(GROUP - k),
            device_id_type=MESH,
        )
        c.start()
        d_copies.append(c)
    for c in d_copies:
        c.wait_recv()
    dense_sum = dsend[0].astype(F32)
    for k in range(1, GROUP):
        dense_sum = dense_sum + drecv[k].astype(F32)

    returned = pltpu.make_async_remote_copy(
        src_ref=back_send.at[others],
        dst_ref=back_recv.at[others],
        send_sem=b_send,
        recv_sem=b_recv,
        device_id=x_peer(1),
        device_id_type=MESH,
    )
    returned.wait_recv()
    expert_rows = back_recv[...].reshape(n_pick, span)
    expert_sum = dot(comb_hi[...], expert_rows) + dot(comb_lo[...], expert_rows)
    mine_cols = pl.ds(pl.multiple_of(tp * span, span), span)
    out = resid[:, mine_cols] + expert_sum[:rows] + mix_gate * dense_sum
    out_ref[...] = out.astype(BF)

    for c in sum(z_copies.values(), []) + x_copies + t_copies + sum(e_copies, []) + h_copies + d_copies:
        c.wait_send()
    arrivals.wait_send()
    returned.wait_send()


def solution(mesh):
    n_ep, n_tp = mesh.shape["ep"], mesh.shape["tp"]

    def shards(*args):
        (
            tokens,
            attn_gain,
            w_query,
            w_key,
            w_value,
            w_forget,
            forget_bias,
            query_gain,
            key_gain,
            cache_pairs,
            cache_cum,
            lengths,
            w_output,
            ffn_gain,
            expert_ids,
            route_weight,
            w_exp_gate,
            w_exp_up,
            w_exp_down,
            shared_gate,
            w_dense_gate,
            w_dense_up,
            w_dense_down,
        ) = args
        rows, width = tokens.shape
        head = query_gain.shape[0]
        slots = cache_pairs.shape[2]
        span = width // n_tp
        n_rows = rows * (w_query.shape[1] // head)
        units = w_dense_gate.shape[0] // n_tp
        n_z = n_ep // GROUP
        ff = w_exp_gate.shape[2]
        n_pick = 2 * n_ep
        operands = (
            tokens,
            attn_gain.reshape(1, -1),
            w_query,
            w_key.T,
            w_value.T,
            w_forget.T,
            forget_bias.reshape(1, -1),
            query_gain.reshape(1, -1),
            key_gain.reshape(1, -1),
            cache_pairs,
            cache_cum,
            lengths.reshape(1, -1),
            w_output,
            ffn_gain.reshape(1, -1),
            expert_ids.T,
            route_weight.T,
            w_exp_gate,
            w_exp_up,
            w_exp_down,
            shared_gate.reshape(-1, 128),
            w_dense_gate,
            w_dense_up,
            w_dense_down,
        )
        dma = pltpu.SemaphoreType.DMA
        vmem = pltpu.VMEM
        like = lambda a: vmem(a.shape, a.dtype)
        scratch = [
            like(tokens),
            like(operands[1]),
            like(w_query),
            like(operands[3]),
            like(operands[4]),
            like(operands[5]),
            like(operands[6]),
            like(operands[7]),
            like(operands[8]),
            vmem((rows, slots, 128), BF),
            like(cache_cum),
            like(operands[11]),
            like(w_output),
            like(operands[13]),
            like(operands[14]),
            like(operands[15]),
            vmem((width, ff), BF),
            vmem((width, ff), BF),
            vmem((ff, width), BF),
            like(operands[19]),
            vmem((n_z, 2, units, width), BF),
            vmem((n_z, units * n_tp, span), BF),
            vmem((rows, slots), F32),
            vmem((n_rows, 256), F32),
            vmem((n_rows, 256), F32),
            vmem((n_rows, slots), F32),
            vmem((n_tp, rows, width), BF),
            vmem((rows, width), F32),
            vmem((GROUP, rows, width), BF),
            vmem((n_ep, 2, width), BF),
            vmem((n_ep, 2, width), BF),
            vmem((n_tp, GROUP * rows, n_z * units), BF),
            vmem((GROUP, rows, span), BF),
            vmem((GROUP, rows, span), BF),
            vmem((n_tp, 2, n_ep, span), BF),
            vmem((n_tp, 2, n_ep, span), BF),
            vmem((n_ep, 2, span), BF),
            vmem((n_ep, 2, span), BF),
            vmem((128, n_pick), BF),
            vmem((128, n_pick), BF),
            vmem((n_pick, 128), BF),
            dma((11,)),
            dma((rows,)),
            dma((8,)),
            dma((3,)),
            dma((2, n_z)),
            dma((2, n_z)),
            dma((n_tp,)),
            dma((n_tp,)),
            dma,
            dma,
            dma((GROUP,)),
            dma((GROUP,)),
            dma((n_tp,)),
            dma((n_tp,)),
            dma((GROUP,)),
            dma((GROUP,)),
            dma((n_tp, 2)),
            dma((n_tp, 2)),
            dma,
            dma,
        ]
        return pl.pallas_call(
            functools.partial(kernel, n_ep, n_tp),
            out_shape=pltpu.VMEM((rows, span), BF),
            in_specs=[pl.BlockSpec(memory_space=pltpu.HBM)] * len(operands),
            out_specs=pl.BlockSpec(memory_space=pltpu.VMEM),
            scratch_shapes=scratch,
            name="layer",
            compiler_params=pltpu.CompilerParams(
                collective_id=0, has_side_effects=True, vmem_limit_bytes=56 * 1024 * 1024
            ),
        )(*operands)

    return jax.shard_map(
        shards,
        mesh=mesh,
        in_specs=(
            P("ep", None),
            P(),
            P(None, "tp"),
            P(None, "tp"),
            P(None, "tp"),
            P(None, "tp"),
            P("tp"),
            P(),
            P(),
            P("ep", "tp", None, None),
            P("ep", "tp", None),
            P("ep"),
            P("tp", None),
            P(),
            P(),
            P(),
            P("ep", None, "tp"),
            P("ep", None, "tp"),
            P("ep", "tp", None),
            P(),
            P("ep", None),
            P("ep", None),
            P("ep", "tp"),
        ),
        out_specs=P("ep", "tp"),
        check_vma=False,
    )
```

```python
import functools

import jax
import jax.numpy as jnp
from jax import lax
from jax.experimental import pallas as pl
from jax.experimental.pallas import tpu as pltpu
from jax.sharding import PartitionSpec as P

EPSILON = 1e-06
MESH = pl.DeviceIdType.MESH
BF = jnp.bfloat16
F32 = jnp.float32
GROUP = 8
NEG = -1e30


def iota(shape, dim):
    return lax.broadcasted_iota(jnp.int32, shape, dim)


def dot(a, b):
    return jnp.dot(a, b, preferred_element_type=F32)


def dot_nt(a, b):
    return lax.dot_general(a, b, (((1,), (1,)), ((), ())), preferred_element_type=F32)


def rms(values):
    return lax.rsqrt(jnp.mean(values * values, axis=-1, keepdims=True) + EPSILON)


def silu(v):
    return v / (1.0 + jnp.exp(-v))


def one_hot(cond):
    return jnp.where(cond, 1.0, 0.0).astype(BF)


def kernel(
    n_ep,
    n_tp,
    tokens_h,
    attn_gain_h,
    w_query_h,
    w_key_h,
    w_value_h,
    w_forget_h,
    forget_bias_h,
    query_gain_h,
    key_gain_h,
    cache_h,
    cum_h,
    lengths_h,
    w_output_h,
    ffn_gain_h,
    ids_h,
    route_h,
    w_gate_h,
    w_up_h,
    w_down_h,
    shared_gate_h,
    dense_gate_h,
    dense_up_h,
    dense_down_h,
    out_ref,
    tok,
    again,
    wq,
    wk,
    wv,
    wf,
    fb,
    qg,
    kg,
    cache,
    cum,
    lens,
    wo,
    fgain,
    ids,
    route,
    wg,
    wu,
    wd,
    sg,
    gz,
    dz,
    bias_rows,
    q_rows,
    mix_rows,
    scores,
    xr,
    resid,
    dt,
    send_rows,
    recv_rows,
    hx,
    dsend,
    drecv,
    esend,
    erecv,
    back_send,
    back_recv,
    comb_hi,
    comb_lo,
    pick,
    load_sem,
    cache_sem,
    weight_sem,
    z_local_sem,
    z_send,
    z_recv,
    x_send,
    x_recv,
    a_send,
    a_recv,
    t_send,
    t_recv,
    h_send,
    h_recv,
    d_send,
    d_recv,
    e_send,
    e_recv,
    b_send,
    b_recv,
):
    ep = lax.axis_index("ep")
    tp = lax.axis_index("tp")
    rows, width = tok.shape
    n_z = n_ep // GROUP
    g = lax.rem(ep, GROUP)
    base = ep - g
    head = qg.shape[1]
    span = width // n_tp
    units = gz.shape[2]

    z = ep // GROUP
    far_first = [n_z // 2]
    for k in range(1, n_z // 2):
        far_first += [n_z // 2 - k, n_z // 2 + k]
    far_first += [0]
    parts = 2
    part_z = n_z // parts
    part_slots = n_ep // parts

    def ep_peer(far, low):
        return lax.rem(z + far, n_z) * GROUP + lax.rem(g + low, GROUP)

    def exchange(half, source, target, send_sem, recv_sem, back):
        for i in range(part_z * half, part_z * (half + 1)):
            far = far_first[i]

            def one(low, carry):
                if back:
                    to = ep_peer(n_z - far, GROUP - low)
                else:
                    to = ep_peer(far, low)
                pltpu.make_async_remote_copy(
                    src_ref=source.at[GROUP * i + low],
                    dst_ref=target.at[GROUP * i + low],
                    send_sem=send_sem,
                    recv_sem=recv_sem,
                    device_id={"ep": to, "tp": tp},
                    device_id_type=MESH,
                ).start()
                return carry

            lax.fori_loop(0 if far else 1, GROUP, one, 0)

    own_slot = n_ep - GROUP

    def x_peer(k):
        return {"ep": ep, "tp": lax.rem(tp + k, n_tp)}

    def group_peer(k):
        return {"ep": base + lax.rem(g + k, GROUP), "tp": tp}

    def z_peer(k):
        return {"ep": lax.rem(ep + GROUP * k, n_ep), "tp": tp}

    small = [
        (tokens_h, tok),
        (attn_gain_h, again),
        (w_query_h, wq),
        (w_key_h, wk),
        (w_value_h, wv),
        (w_forget_h, wf),
        (forget_bias_h, fb),
        (query_gain_h, qg),
        (key_gain_h, kg),
        (cum_h, cum),
        (lengths_h, lens),
    ]
    loads = [pltpu.make_async_copy(s, d, load_sem.at[i]) for i, (s, d) in enumerate(small)]
    for c in loads:
        c.start()
    quarter = pl.ds(pl.multiple_of(tp * units, units), units)
    own_dense = [
        pltpu.make_async_copy(dense_gate_h.at[quarter], gz.at[0, 0], z_local_sem.at[0]),
        pltpu.make_async_copy(dense_up_h.at[quarter], gz.at[0, 1], z_local_sem.at[1]),
        pltpu.make_async_copy(dense_down_h, dz.at[0], z_local_sem.at[2]),
    ]
    for c in own_dense:
        c.start()

    cache_loads = []
    for s in range(rows):
        c = pltpu.make_async_copy(
            cache_h.at[s, 0], cache.at[s], cache_sem.at[s]
        )
        c.start()
        cache_loads.append(c)
    barrier = pltpu.get_barrier_semaphore()

    def greet(k, carry):
        pl.semaphore_signal(
            barrier,
            inc=1,
            device_id={"ep": lax.rem(ep + k, n_ep), "tp": tp},
            device_id_type=MESH,
        )
        return carry

    lax.fori_loop(1, n_ep, greet, 0)
    for k in range(1, n_tp):
        pl.semaphore_signal(barrier, inc=1, device_id=x_peer(k), device_id_type=MESH)
    later = [
        (w_output_h, wo),
        (ffn_gain_h, fgain),
        (ids_h, ids),
        (route_h, route),
        (shared_gate_h, sg),
        (w_gate_h.at[0], wg),
        (w_up_h.at[0], wu),
        (w_down_h.at[0], wd),
    ]
    late_loads = [pltpu.make_async_copy(s, d, weight_sem.at[i]) for i, (s, d) in enumerate(later)]
    for c in late_loads[:5]:
        c.start()
    z_copies = {}

    def pass_on(t):
        for come, go, to in ((t, t + 1, 1), ((n_z - t) % n_z, n_z - 1 - t, n_z - 1)):
            if (t < n_z // 2) if to == 1 else (t < n_z - 1 - n_z // 2):
                if t:
                    for c in z_copies[come]:
                        c.wait_recv()
                z_copies[go] = [
                    pltpu.make_async_remote_copy(
                        src_ref=held.at[come],
                        dst_ref=held.at[go],
                        send_sem=z_send.at[i, go],
                        recv_sem=z_recv.at[i, go],
                        device_id=z_peer(to),
                        device_id_type=MESH,
                    )
                    for i, held in enumerate((gz, dz))
                ]
                for c in z_copies[go]:
                    c.start()

    for c in loads:
        c.wait()
    tokens_f = tok[...].astype(F32)
    normed = (tokens_f * rms(tokens_f) * again[...]).astype(BF)
    query_raw = dot(normed, wq[...])
    key_raw = dot_nt(normed, wk[...])
    value_new = dot_nt(normed, wv[...]).astype(BF)
    forget = jnp.sum(normed.astype(F32) * wf[...].astype(F32), axis=1, keepdims=True)
    forget = forget + fb[...]
    log_gate = jnp.minimum(forget, 0.0) - jnp.log1p(jnp.exp(-jnp.abs(forget)))

    lane_q = iota((rows, span), 1)
    squares = query_raw * query_raw
    scale = jnp.zeros((rows, span), F32)
    for h in range(span // head):
        here = lane_q // head == h
        total = jnp.sum(jnp.where(here, squares, 0.0), axis=1, keepdims=True)
        scale = jnp.where(here, lax.rsqrt(total / head + EPSILON), scale)
    gains = jnp.concatenate([qg[...]] * (span // head), axis=1)
    queries = (query_raw * scale * gains).astype(BF).astype(F32) * head ** (-0.5)
    queries = queries.astype(BF)
    key_new = (key_raw * rms(key_raw) * kg[...]).astype(BF)

    heads = span // head
    n_rows = rows * heads
    row_r = iota((n_rows, 256), 0)
    lane_r = iota((n_rows, 256), 1)
    seq_of = one_hot(iota((n_rows, rows), 0) // heads == iota((n_rows, rows), 1))
    own_half = lane_r // 128 == (row_r // heads) % 2
    own_head = lane_r // head == row_r % heads
    low = own_half & (lane_r % 128 < head)
    high = own_half & (lane_r % 128 >= head)
    fold = one_hot(iota((256, 256), 0) % head == iota((256, 256), 1) % head)
    spread = one_hot(iota((head, 256), 0) == iota((head, 256), 1) % head)

    q_all = jnp.where(own_head, dot(seq_of, queries), 0.0).astype(BF)
    q_wide = jnp.where(low, dot(q_all, fold), 0.0)
    q_rows[...] = q_wide
    key_wide = dot(seq_of, dot(key_new, spread).astype(BF))
    own_score = jnp.sum(q_wide * key_wide, axis=1, keepdims=True)
    value_wide = jnp.where(high, dot(seq_of, dot(value_new, spread).astype(BF)), 0.0)

    cum_2d = cum[...].reshape(rows, cum.shape[2])
    slots = cum_2d.shape[1]
    lens_f = lens[...].astype(F32)
    lens_col = jnp.sum(
        jnp.where(iota((rows, rows), 0) == iota((rows, rows), 1), lens_f, 0.0),
        axis=1,
        keepdims=True,
    )
    position = iota((rows, slots), 1).astype(F32)
    last_cum = jnp.sum(jnp.where(position == lens_col - 1.0, cum_2d, 0.0), axis=1, keepdims=True)
    now_cum = last_cum + log_gate
    bias_rows[...] = jnp.where(position < lens_col, now_cum - cum_2d, NEG)

    pair = 2 * heads
    per = 6
    batches = rows // 2 // per
    batch_rows = per * pair

    def both_of(p, c):
        at = pl.ds(256 * c, 256)
        return jnp.concatenate([cache[2 * p, at, :], cache[2 * p + 1, at, :]], axis=1)

    def score_batch(b):
        for i in range(2 * per * b, 2 * per * (b + 1)):
            cache_loads[i].wait()
        for p in range(per * b, per * (b + 1)):
            q_pair = q_rows[pl.ds(pair * p, pair), :].astype(BF)
            for c in range(slots // 256):
                scores[pl.ds(pair * p, pair), pl.ds(256 * c, 256)] = dot_nt(q_pair, both_of(p, c))

    first = iota((pair, slots), 0) < heads
    totals = []
    own_parts = []
    score_batch(0)
    pl.semaphore_wait(barrier, n_ep - 1 + n_tp - 1)
    for c in own_dense:
        c.wait()
    pass_on(0)
    for b in range(batches):
        if b + 1 < batches:
            score_batch(b + 1)
        if b == 0:
            for c in late_loads[5:]:
                c.start()
        decay = jnp.concatenate(
            [
                jnp.where(
                    first,
                    jnp.broadcast_to(bias_rows[pl.ds(2 * p, 1), :], (pair, slots)),
                    jnp.broadcast_to(bias_rows[pl.ds(2 * p + 1, 1), :], (pair, slots)),
                )
                for p in range(per * b, per * (b + 1))
            ],
            axis=0,
        )
        here = pl.ds(batch_rows * b, batch_rows)
        score = scores[here, :] + decay
        own = own_score[batch_rows * b : batch_rows * (b + 1)]
        peak = jnp.maximum(jnp.max(score, axis=1, keepdims=True), own)
        past = jnp.exp(score - peak)
        own_exp = jnp.exp(own - peak)
        totals.append(jnp.sum(past, axis=1, keepdims=True) + own_exp)
        own_parts.append(own_exp)
        prob = past.astype(BF)
        for i in range(per):
            p = per * b + i
            prob_pair = prob[pair * i : pair * (i + 1)]
            total = dot(prob_pair[:, :256], both_of(p, 0))
            for c in range(1, slots // 256):
                total = total + dot(prob_pair[:, 256 * c : 256 * (c + 1)], both_of(p, c))
            mix_rows[pl.ds(pair * p, pair), :] = total
    inverse = 1.0 / jnp.concatenate(totals, axis=0)
    mixed = jnp.where(high, mix_rows[...], 0.0)
    mixed = (mixed + jnp.concatenate(own_parts, axis=0) * value_wide) * inverse
    by_head = jnp.where(own_head, dot(mixed.astype(BF), fold), 0.0).astype(BF)
    to_seq = one_hot(iota((rows, n_rows), 1) // heads == iota((rows, n_rows), 0))
    head_mix = dot(to_seq, by_head).astype(BF)
    for c in late_loads[:5]:
        c.wait()
    xr[0] = dot(head_mix, wo[...]).astype(BF)
    x_copies = []
    for k in (2, 1, 3):
        c = pltpu.make_async_remote_copy(
            src_ref=xr.at[0],
            dst_ref=xr.at[k],
            send_sem=x_send.at[k],
            recv_sem=x_recv.at[k],
            device_id=x_peer(k),
            device_id_type=MESH,
        )
        c.start()
        x_copies.append(c)

    pass_on(1)

    n_pick = 2 * n_ep
    tokens_all = ids.shape[1]
    window = 256
    first_lane = ep * rows
    start = jnp.minimum(first_lane // 128, (tokens_all - window) // 128) * 128
    offset = first_lane - start
    pick_lanes = iota((window, 128), 0) == iota((window, 128), 1) + offset
    pick_lanes = jnp.where(pick_lanes & (iota((window, 128), 1) < rows), 1.0, 0.0)
    lanes = pl.ds(pl.multiple_of(start, 128), window)
    both = jnp.concatenate([ids[:, lanes].astype(F32), route[:, lanes]], axis=0)
    mine = jnp.dot(both, pick_lanes, precision=lax.Precision.HIGHEST, preferred_element_type=F32)
    lane_p = iota((n_pick, 128), 1)
    slot_of = iota((n_pick, 128), 0) // 2
    far_of = jnp.zeros((n_pick, 128), jnp.int32)
    for i, far in enumerate(far_first):
        far_of = jnp.where(slot_of // GROUP == i, far, far_of)
    expert = lax.rem(z + far_of, n_z) * GROUP + lax.rem(g + slot_of % GROUP, GROUP)
    expert = expert.astype(F32)
    live = lane_p < rows
    hit_0 = (mine[0:1] == expert) & live
    hit_1 = (mine[1:2] == expert) & live
    hit = one_hot(hit_0 | hit_1)
    rank = dot(hit, one_hot(iota((128, 128), 0) <= iota((128, 128), 1)))
    slot = (iota((n_pick, 128), 0) % 2 + 1).astype(F32)
    picked = jnp.where((rank == slot) & (hit.astype(F32) > 0.5), 1.0, 0.0)
    pick[...] = picked.astype(BF)
    weight = jnp.where(hit_0, mine[2:3], 0.0) + jnp.where(hit_1, mine[3:4], 0.0)
    combine = (picked * weight).T
    combine_hi = combine.astype(BF)
    comb_hi[...] = combine_hi
    comb_lo[...] = (combine - combine_hi.astype(F32)).astype(BF)

    for c in x_copies:
        c.wait_recv()
    attn_out = xr[0].astype(F32) + xr[1].astype(F32) + xr[2].astype(F32) + xr[3].astype(F32)
    residual = (tok[...].astype(F32) + attn_out).astype(BF).astype(F32)
    resid[...] = residual
    normed_two = (residual * rms(residual) * fgain[...]).astype(BF)
    dt[0] = normed_two
    gate_row = sg[...].astype(F32)
    gate_row = jnp.concatenate([gate_row[i : i + 1] for i in range(width // 128)], axis=1)
    mix_gate = jnp.sum(normed_two.astype(F32) * gate_row, axis=1, keepdims=True)
    mix_gate = 1.0 / (1.0 + jnp.exp(-mix_gate))
    for half in range(parts):
        at = pl.ds(2 * part_slots * half, 2 * part_slots)
        packed = dot(pick[at, :rows], normed_two).astype(BF)
        send_rows[pl.ds(part_slots * half, part_slots)] = packed.reshape(part_slots, 2, width)
        exchange(half, send_rows, recv_rows, a_send, a_recv, False)
    recv_rows[own_slot] = send_rows[own_slot]
    t_copies = []
    for k in range(1, GROUP):
        c = pltpu.make_async_remote_copy(
            src_ref=dt.at[0],
            dst_ref=dt.at[k],
            send_sem=t_send.at[k],
            recv_sem=t_recv.at[k],
            device_id=group_peer(k),
            device_id_type=MESH,
        )
        c.start()
        t_copies.append(c)

    pass_on(2)
    pass_on(3)

    for c in late_loads[5:]:
        c.wait()
    others = pl.ds(0, n_ep - 1)
    arrivals = pltpu.make_async_remote_copy(
        src_ref=send_rows.at[others],
        dst_ref=recv_rows.at[others],
        send_sem=a_send,
        recv_sem=a_recv,
        device_id=x_peer(1),
        device_id_type=MESH,
    )
    arrivals.wait_recv()
    routed = recv_rows[...].reshape(n_pick, width)
    hidden = (silu(dot(routed, wg[...])) * dot(routed, wu[...])).astype(BF)
    e_copies = [[], []]
    for k in (2, 1, 3, 0):
        column = pl.ds(pl.multiple_of(lax.rem(tp + k, n_tp) * span, span), span)
        part = dot(hidden, wd[:, column]).astype(BF)
        esend[k] = part.reshape(parts, n_pick // parts, span)
        if k:
            for half in range(parts):
                c = pltpu.make_async_remote_copy(
                    src_ref=esend.at[k, half],
                    dst_ref=erecv.at[k, half],
                    send_sem=e_send.at[k, half],
                    recv_sem=e_recv.at[k, half],
                    device_id=x_peer(k),
                    device_id_type=MESH,
                )
                e_copies[half].append(c)
            e_copies[0][-1].start()
    for c in e_copies[1]:
        c.start()

    for come in (n_z // 2, n_z - (n_z - 1 - n_z // 2)):
        for c in z_copies[come]:
            c.wait_recv()
    for c in t_copies:
        c.wait_recv()
    group_rows = dt[...].reshape(GROUP * rows, width)
    dense_w = n_z * units
    dense_gate = dot_nt(group_rows, gz[:, 0].reshape(dense_w, width))
    dense_up = dot_nt(group_rows, gz[:, 1].reshape(dense_w, width))
    hx[0] = (silu(dense_gate) * dense_up).astype(BF)
    h_copies = []
    for k in (2, 1, 3):
        c = pltpu.make_async_remote_copy(
            src_ref=hx.at[0],
            dst_ref=hx.at[k],
            send_sem=h_send.at[k],
            recv_sem=h_recv.at[k],
            device_id=x_peer(k),
            device_id_type=MESH,
        )
        c.start()
        h_copies.append(c)

    for half in range(parts):
        for c in e_copies[half]:
            c.wait_recv()
        summed = esend[0, half].astype(F32) + erecv[1, half].astype(F32)
        summed = summed + erecv[2, half].astype(F32) + erecv[3, half].astype(F32)
        at = pl.ds(part_slots * half, part_slots)
        back_send[at] = summed.astype(BF).reshape(part_slots, 2, span)
        exchange(half, back_send, back_recv, b_send, b_recv, True)
    back_recv[own_slot] = back_send[own_slot]

    for c in h_copies:
        c.wait_recv()
    dense_part = jnp.zeros((GROUP * rows, span), F32)
    for k in range(n_tp):
        owner = lax.rem(tp + n_tp - k, n_tp)
        part = dz[:, pl.ds(pl.multiple_of(owner * units, units), units), :]
        dense_part = dense_part + dot(hx[k], part.reshape(dense_w, span))
    dsend[...] = dense_part.astype(BF).reshape(GROUP, rows, span)
    d_copies = []
    for k in range(1, GROUP):
        c = pltpu.make_async_remote_copy(
            src_ref=dsend.at[k],
            dst_ref=drecv.at[k],
            send_sem=d_send.at[k],
            recv_sem=d_recv.at[k],
            device_id=group_peer(GROUP - k),
            device_id_type=MESH,
        )
        c.start()
        d_copies.append(c)
    for c in d_copies:
        c.wait_recv()
    dense_sum = dsend[0].astype(F32)
    for k in range(1, GROUP):
        dense_sum = dense_sum + drecv[k].astype(F32)

    returned = pltpu.make_async_remote_copy(
        src_ref=back_send.at[others],
        dst_ref=back_recv.at[others],
        send_sem=b_send,
        recv_sem=b_recv,
        device_id=x_peer(1),
        device_id_type=MESH,
    )
    returned.wait_recv()
    expert_rows = back_recv[...].reshape(n_pick, span)
    expert_sum = dot(comb_hi[...], expert_rows) + dot(comb_lo[...], expert_rows)
    mine_cols = pl.ds(pl.multiple_of(tp * span, span), span)
    out = resid[:, mine_cols] + expert_sum[:rows] + mix_gate * dense_sum
    out_ref[...] = out.astype(BF)

    for c in sum(z_copies.values(), []) + x_copies + t_copies + sum(e_copies, []) + h_copies + d_copies:
        c.wait_send()
    arrivals.wait_send()
    returned.wait_send()


def solution(mesh):
    n_ep, n_tp = mesh.shape["ep"], mesh.shape["tp"]

    def shards(*args):
        (
            tokens,
            attn_gain,
            w_query,
            w_key,
            w_value,
            w_forget,
            forget_bias,
            query_gain,
            key_gain,
            cache_pairs,
            cache_cum,
            lengths,
            w_output,
            ffn_gain,
            expert_ids,
            route_weight,
            w_exp_gate,
            w_exp_up,
            w_exp_down,
            shared_gate,
            w_dense_gate,
            w_dense_up,
            w_dense_down,
        ) = args
        rows, width = tokens.shape
        head = query_gain.shape[0]
        slots = cache_pairs.shape[2]
        span = width // n_tp
        n_rows = rows * (w_query.shape[1] // head)
        units = w_dense_gate.shape[0] // n_tp
        n_z = n_ep // GROUP
        ff = w_exp_gate.shape[2]
        n_pick = 2 * n_ep
        operands = (
            tokens,
            attn_gain.reshape(1, -1),
            w_query,
            w_key.T,
            w_value.T,
            w_forget.T,
            forget_bias.reshape(1, -1),
            query_gain.reshape(1, -1),
            key_gain.reshape(1, -1),
            cache_pairs,
            cache_cum,
            lengths.reshape(1, -1),
            w_output,
            ffn_gain.reshape(1, -1),
            expert_ids.T,
            route_weight.T,
            w_exp_gate,
            w_exp_up,
            w_exp_down,
            shared_gate.reshape(-1, 128),
            w_dense_gate,
            w_dense_up,
            w_dense_down,
        )
        dma = pltpu.SemaphoreType.DMA
        vmem = pltpu.VMEM
        like = lambda a: vmem(a.shape, a.dtype)
        scratch = [
            like(tokens),
            like(operands[1]),
            like(w_query),
            like(operands[3]),
            like(operands[4]),
            like(operands[5]),
            like(operands[6]),
            like(operands[7]),
            like(operands[8]),
            vmem((rows, slots, 128), BF),
            like(cache_cum),
            like(operands[11]),
            like(w_output),
            like(operands[13]),
            like(operands[14]),
            like(operands[15]),
            vmem((width, ff), BF),
            vmem((width, ff), BF),
            vmem((ff, width), BF),
            like(operands[19]),
            vmem((n_z, 2, units, width), BF),
            vmem((n_z, units * n_tp, span), BF),
            vmem((rows, slots), F32),
            vmem((n_rows, 256), F32),
            vmem((n_rows, 256), F32),
            vmem((n_rows, slots), F32),
            vmem((n_tp, rows, width), BF),
            vmem((rows, width), F32),
            vmem((GROUP, rows, width), BF),
            vmem((n_ep, 2, width), BF),
            vmem((n_ep, 2, width), BF),
            vmem((n_tp, GROUP * rows, n_z * units), BF),
            vmem((GROUP, rows, span), BF),
            vmem((GROUP, rows, span), BF),
            vmem((n_tp, 2, n_ep, span), BF),
            vmem((n_tp, 2, n_ep, span), BF),
            vmem((n_ep, 2, span), BF),
            vmem((n_ep, 2, span), BF),
            vmem((128, n_pick), BF),
            vmem((128, n_pick), BF),
            vmem((n_pick, 128), BF),
            dma((11,)),
            dma((rows,)),
            dma((8,)),
            dma((3,)),
            dma((2, n_z)),
            dma((2, n_z)),
            dma((n_tp,)),
            dma((n_tp,)),
            dma,
            dma,
            dma((GROUP,)),
            dma((GROUP,)),
            dma((n_tp,)),
            dma((n_tp,)),
            dma((GROUP,)),
            dma((GROUP,)),
            dma((n_tp, 2)),
            dma((n_tp, 2)),
            dma,
            dma,
        ]
        return pl.pallas_call(
            functools.partial(kernel, n_ep, n_tp),
            out_shape=pltpu.VMEM((rows, span), BF),
            in_specs=[pl.BlockSpec(memory_space=pltpu.HBM)] * len(operands),
            out_specs=pl.BlockSpec(memory_space=pltpu.VMEM),
            scratch_shapes=scratch,
            name="layer",
            compiler_params=pltpu.CompilerParams(
                collective_id=0, has_side_effects=True, vmem_limit_bytes=56 * 1024 * 1024
            ),
        )(*operands)

    return jax.shard_map(
        shards,
        mesh=mesh,
        in_specs=(
            P("ep", None),
            P(),
            P(None, "tp"),
            P(None, "tp"),
            P(None, "tp"),
            P(None, "tp"),
            P("tp"),
            P(),
            P(),
            P("ep", "tp", None, None),
            P("ep", "tp", None),
            P("ep"),
            P("tp", None),
            P(),
            P(),
            P(),
            P("ep", None, "tp"),
            P("ep", None, "tp"),
            P("ep", "tp", None),
            P(),
            P("ep", None),
            P("ep", None),
            P("ep", "tp"),
        ),
        out_specs=P("ep", "tp"),
        check_vma=False,
    )
```

```python
import functools

import jax
import jax.numpy as jnp
from jax import lax
from jax.experimental import pallas as pl
from jax.experimental.pallas import tpu as pltpu
from jax.sharding import PartitionSpec as P

EPSILON = 1e-06
MESH = pl.DeviceIdType.MESH
BF = jnp.bfloat16
F32 = jnp.float32
GROUP = 8
NEG = -1e30


def iota(shape, dim):
    return lax.broadcasted_iota(jnp.int32, shape, dim)


def dot(a, b):
    return jnp.dot(a, b, preferred_element_type=F32)


def dot_nt(a, b):
    return lax.dot_general(a, b, (((1,), (1,)), ((), ())), preferred_element_type=F32)


def rms(values):
    return lax.rsqrt(jnp.mean(values * values, axis=-1, keepdims=True) + EPSILON)


def silu(v):
    return v / (1.0 + jnp.exp(-v))


def one_hot(cond):
    return jnp.where(cond, 1.0, 0.0).astype(BF)


def kernel(
    n_ep,
    n_tp,
    tokens_h,
    attn_gain_h,
    w_query_h,
    w_key_h,
    w_value_h,
    w_forget_h,
    forget_bias_h,
    query_gain_h,
    key_gain_h,
    cache_h,
    cum_h,
    lengths_h,
    w_output_h,
    ffn_gain_h,
    ids_h,
    route_h,
    w_gate_h,
    w_up_h,
    w_down_h,
    shared_gate_h,
    dense_gate_h,
    dense_up_h,
    dense_down_h,
    out_ref,
    tok,
    again,
    wq,
    wk,
    wv,
    wf,
    fb,
    qg,
    kg,
    cache,
    cum,
    lens,
    wo,
    fgain,
    ids,
    route,
    wg,
    wu,
    wd,
    sg,
    gz,
    dz,
    bias_rows,
    q_rows,
    mix_rows,
    scores,
    xr,
    resid,
    dt,
    send_rows,
    recv_rows,
    hx,
    dsend,
    drecv,
    esend,
    erecv,
    back_send,
    back_recv,
    comb_hi,
    comb_lo,
    pick,
    load_sem,
    cache_sem,
    weight_sem,
    z_local_sem,
    z_send,
    z_recv,
    x_send,
    x_recv,
    a_send,
    a_recv,
    t_send,
    t_recv,
    h_send,
    h_recv,
    d_send,
    d_recv,
    e_send,
    e_recv,
    b_send,
    b_recv,
):
    ep = lax.axis_index("ep")
    tp = lax.axis_index("tp")
    rows, width = tok.shape
    n_z = n_ep // GROUP
    g = lax.rem(ep, GROUP)
    base = ep - g
    head = qg.shape[1]
    span = width // n_tp
    units = gz.shape[2]

    z = ep // GROUP
    far_first = [n_z // 2]
    for k in range(1, n_z // 2):
        far_first += [n_z // 2 - k, n_z // 2 + k]
    far_first += [0]
    parts = 2
    part_z = n_z // parts
    part_slots = n_ep // parts

    def ep_peer(far, low):
        return lax.rem(z + far, n_z) * GROUP + lax.rem(g + low, GROUP)

    def exchange(half, source, target, send_sem, recv_sem, back):
        for i in range(part_z * half, part_z * (half + 1)):
            far = far_first[i]

            def one(low, carry):
                if back:
                    to = ep_peer(n_z - far, GROUP - low)
                else:
                    to = ep_peer(far, low)
                pltpu.make_async_remote_copy(
                    src_ref=source.at[GROUP * i + low],
                    dst_ref=target.at[GROUP * i + low],
                    send_sem=send_sem,
                    recv_sem=recv_sem,
                    device_id={"ep": to, "tp": tp},
                    device_id_type=MESH,
                ).start()
                return carry

            lax.fori_loop(0 if far else 1, GROUP, one, 0)

    own_slot = n_ep - GROUP

    def x_peer(k):
        return {"ep": ep, "tp": lax.rem(tp + k, n_tp)}

    def group_peer(k):
        return {"ep": base + lax.rem(g + k, GROUP), "tp": tp}

    def z_peer(k):
        return {"ep": lax.rem(ep + GROUP * k, n_ep), "tp": tp}

    small = [
        (tokens_h, tok),
        (attn_gain_h, again),
        (w_query_h, wq),
        (w_key_h, wk),
        (w_value_h, wv),
        (w_forget_h, wf),
        (forget_bias_h, fb),
        (query_gain_h, qg),
        (key_gain_h, kg),
        (cum_h, cum),
        (lengths_h, lens),
    ]
    loads = [pltpu.make_async_copy(s, d, load_sem.at[i]) for i, (s, d) in enumerate(small)]
    for c in loads:
        c.start()
    quarter = pl.ds(pl.multiple_of(tp * units, units), units)
    own_dense = [
        pltpu.make_async_copy(dense_gate_h.at[quarter], gz.at[0, 0], z_local_sem.at[0]),
        pltpu.make_async_copy(dense_up_h.at[quarter], gz.at[0, 1], z_local_sem.at[1]),
        pltpu.make_async_copy(dense_down_h, dz.at[0], z_local_sem.at[2]),
    ]
    for c in own_dense:
        c.start()

    cache_loads = []
    for s in range(rows):
        c = pltpu.make_async_copy(
            cache_h.at[s, 0], cache.at[s], cache_sem.at[s]
        )
        c.start()
        cache_loads.append(c)
    barrier = pltpu.get_barrier_semaphore()

    def greet(k, carry):
        pl.semaphore_signal(
            barrier,
            inc=1,
            device_id={"ep": lax.rem(ep + k, n_ep), "tp": tp},
            device_id_type=MESH,
        )
        return carry

    lax.fori_loop(1, n_ep, greet, 0)
    for k in range(1, n_tp):
        pl.semaphore_signal(barrier, inc=1, device_id=x_peer(k), device_id_type=MESH)
    later = [
        (w_output_h, wo),
        (ffn_gain_h, fgain),
        (ids_h, ids),
        (route_h, route),
        (shared_gate_h, sg),
        (w_gate_h.at[0], wg),
        (w_up_h.at[0], wu),
        (w_down_h.at[0], wd),
    ]
    late_loads = [pltpu.make_async_copy(s, d, weight_sem.at[i]) for i, (s, d) in enumerate(later)]
    for c in late_loads[:5]:
        c.start()
    z_copies = {}

    def pass_on(t):
        for come, go, to in ((t, t + 1, 1), ((n_z - t) % n_z, n_z - 1 - t, n_z - 1)):
            if (t < n_z // 2) if to == 1 else (t < n_z - 1 - n_z // 2):
                if t:
                    for c in z_copies[come]:
                        c.wait_recv()
                z_copies[go] = [
                    pltpu.make_async_remote_copy(
                        src_ref=held.at[come],
                        dst_ref=held.at[go],
                        send_sem=z_send.at[i, go],
                        recv_sem=z_recv.at[i, go],
                        device_id=z_peer(to),
                        device_id_type=MESH,
                    )
                    for i, held in enumerate((gz, dz))
                ]
                for c in z_copies[go]:
                    c.start()

    for c in loads:
        c.wait()
    tokens_f = tok[...].astype(F32)
    normed = (tokens_f * rms(tokens_f) * again[...]).astype(BF)
    query_raw = dot(normed, wq[...])
    key_raw = dot_nt(normed, wk[...])
    value_new = dot_nt(normed, wv[...]).astype(BF)
    forget = jnp.sum(normed.astype(F32) * wf[...].astype(F32), axis=1, keepdims=True)
    forget = forget + fb[...]
    log_gate = jnp.minimum(forget, 0.0) - jnp.log1p(jnp.exp(-jnp.abs(forget)))

    lane_q = iota((rows, span), 1)
    squares = query_raw * query_raw
    scale = jnp.zeros((rows, span), F32)
    for h in range(span // head):
        here = lane_q // head == h
        total = jnp.sum(jnp.where(here, squares, 0.0), axis=1, keepdims=True)
        scale = jnp.where(here, lax.rsqrt(total / head + EPSILON), scale)
    gains = jnp.concatenate([qg[...]] * (span // head), axis=1)
    queries = (query_raw * scale * gains).astype(BF).astype(F32) * head ** (-0.5)
    queries = queries.astype(BF)
    key_new = (key_raw * rms(key_raw) * kg[...]).astype(BF)

    heads = span // head
    n_rows = rows * heads
    row_r = iota((n_rows, 256), 0)
    lane_r = iota((n_rows, 256), 1)
    seq_of = one_hot(iota((n_rows, rows), 0) // heads == iota((n_rows, rows), 1))
    own_half = lane_r // 128 == (row_r // heads) % 2
    own_head = lane_r // head == row_r % heads
    low = own_half & (lane_r % 128 < head)
    high = own_half & (lane_r % 128 >= head)
    fold = one_hot(iota((256, 256), 0) % head == iota((256, 256), 1) % head)
    spread = one_hot(iota((head, 256), 0) == iota((head, 256), 1) % head)

    q_all = jnp.where(own_head, dot(seq_of, queries), 0.0).astype(BF)
    q_wide = jnp.where(low, dot(q_all, fold), 0.0)
    q_rows[...] = q_wide
    key_wide = dot(seq_of, dot(key_new, spread).astype(BF))
    own_score = jnp.sum(q_wide * key_wide, axis=1, keepdims=True)
    value_wide = jnp.where(high, dot(seq_of, dot(value_new, spread).astype(BF)), 0.0)

    cum_2d = cum[...].reshape(rows, cum.shape[2])
    slots = cum_2d.shape[1]
    lens_f = lens[...].astype(F32)
    lens_col = jnp.sum(
        jnp.where(iota((rows, rows), 0) == iota((rows, rows), 1), lens_f, 0.0),
        axis=1,
        keepdims=True,
    )
    position = iota((rows, slots), 1).astype(F32)
    last_cum = jnp.sum(jnp.where(position == lens_col - 1.0, cum_2d, 0.0), axis=1, keepdims=True)
    now_cum = last_cum + log_gate
    bias_rows[...] = jnp.where(position < lens_col, now_cum - cum_2d, NEG)

    pair = 2 * heads
    per = 6
    batches = rows // 2 // per
    batch_rows = per * pair

    def both_of(p, c):
        at = pl.ds(256 * c, 256)
        return jnp.concatenate([cache[2 * p, at, :], cache[2 * p + 1, at, :]], axis=1)

    def score_batch(b):
        for i in range(2 * per * b, 2 * per * (b + 1)):
            cache_loads[i].wait()
        for p in range(per * b, per * (b + 1)):
            q_pair = q_rows[pl.ds(pair * p, pair), :].astype(BF)
            for c in range(slots // 256):
                scores[pl.ds(pair * p, pair), pl.ds(256 * c, 256)] = dot_nt(q_pair, both_of(p, c))

    first = iota((pair, slots), 0) < heads
    totals = []
    own_parts = []
    score_batch(0)
    pl.semaphore_wait(barrier, n_ep - 1 + n_tp - 1)
    for c in own_dense:
        c.wait()
    pass_on(0)
    for b in range(batches):
        if b + 1 < batches:
            score_batch(b + 1)
        if b == 0:
            for c in late_loads[5:]:
                c.start()
        decay = jnp.concatenate(
            [
                jnp.where(
                    first,
                    jnp.broadcast_to(bias_rows[pl.ds(2 * p, 1), :], (pair, slots)),
                    jnp.broadcast_to(bias_rows[pl.ds(2 * p + 1, 1), :], (pair, slots)),
                )
                for p in range(per * b, per * (b + 1))
            ],
            axis=0,
        )
        here = pl.ds(batch_rows * b, batch_rows)
        score = scores[here, :] + decay
        own = own_score[batch_rows * b : batch_rows * (b + 1)]
        peak = jnp.maximum(jnp.max(score, axis=1, keepdims=True), own)
        past = jnp.exp(score - peak)
        own_exp = jnp.exp(own - peak)
        totals.append(jnp.sum(past, axis=1, keepdims=True) + own_exp)
        own_parts.append(own_exp)
        prob = past.astype(BF)
        for i in range(per):
            p = per * b + i
            prob_pair = prob[pair * i : pair * (i + 1)]
            total = dot(prob_pair[:, :256], both_of(p, 0))
            for c in range(1, slots // 256):
                total = total + dot(prob_pair[:, 256 * c : 256 * (c + 1)], both_of(p, c))
            mix_rows[pl.ds(pair * p, pair), :] = total
    inverse = 1.0 / jnp.concatenate(totals, axis=0)
    mixed = jnp.where(high, mix_rows[...], 0.0)
    mixed = (mixed + jnp.concatenate(own_parts, axis=0) * value_wide) * inverse
    by_head = jnp.where(own_head, dot(mixed.astype(BF), fold), 0.0).astype(BF)
    to_seq = one_hot(iota((rows, n_rows), 1) // heads == iota((rows, n_rows), 0))
    head_mix = dot(to_seq, by_head).astype(BF)
    for c in late_loads[:5]:
        c.wait()
    xr[0] = dot(head_mix, wo[...]).astype(BF)
    x_copies = []
    for k in (2, 1, 3):
        c = pltpu.make_async_remote_copy(
            src_ref=xr.at[0],
            dst_ref=xr.at[k],
            send_sem=x_send.at[k],
            recv_sem=x_recv.at[k],
            device_id=x_peer(k),
            device_id_type=MESH,
        )
        c.start()
        x_copies.append(c)

    n_pick = 2 * n_ep
    tokens_all = ids.shape[1]
    window = 256
    first_lane = ep * rows
    start = jnp.minimum(first_lane // 128, (tokens_all - window) // 128) * 128
    offset = first_lane - start
    pick_lanes = iota((window, 128), 0) == iota((window, 128), 1) + offset
    pick_lanes = jnp.where(pick_lanes & (iota((window, 128), 1) < rows), 1.0, 0.0)
    lanes = pl.ds(pl.multiple_of(start, 128), window)
    both = jnp.concatenate([ids[:, lanes].astype(F32), route[:, lanes]], axis=0)
    mine = jnp.dot(both, pick_lanes, precision=lax.Precision.HIGHEST, preferred_element_type=F32)
    lane_p = iota((n_pick, 128), 1)
    slot_of = iota((n_pick, 128), 0) // 2
    far_of = jnp.zeros((n_pick, 128), jnp.int32)
    for i, far in enumerate(far_first):
        far_of = jnp.where(slot_of // GROUP == i, far, far_of)
    expert = lax.rem(z + far_of, n_z) * GROUP + lax.rem(g + slot_of % GROUP, GROUP)
    expert = expert.astype(F32)
    live = lane_p < rows
    hit_0 = (mine[0:1] == expert) & live
    hit_1 = (mine[1:2] == expert) & live
    hit = one_hot(hit_0 | hit_1)
    rank = dot(hit, one_hot(iota((128, 128), 0) <= iota((128, 128), 1)))
    slot = (iota((n_pick, 128), 0) % 2 + 1).astype(F32)
    picked = jnp.where((rank == slot) & (hit.astype(F32) > 0.5), 1.0, 0.0)
    pick[...] = picked.astype(BF)
    weight = jnp.where(hit_0, mine[2:3], 0.0) + jnp.where(hit_1, mine[3:4], 0.0)
    combine = (picked * weight).T
    combine_hi = combine.astype(BF)
    comb_hi[...] = combine_hi
    comb_lo[...] = (combine - combine_hi.astype(F32)).astype(BF)

    pass_on(1)
    for c in x_copies:
        c.wait_recv()
    attn_out = xr[0].astype(F32) + xr[1].astype(F32) + xr[2].astype(F32) + xr[3].astype(F32)
    residual = (tok[...].astype(F32) + attn_out).astype(BF).astype(F32)
    resid[...] = residual
    normed_two = (residual * rms(residual) * fgain[...]).astype(BF)
    dt[0] = normed_two
    gate_row = sg[...].astype(F32)
    gate_row = jnp.concatenate([gate_row[i : i + 1] for i in range(width // 128)], axis=1)
    mix_gate = jnp.sum(normed_two.astype(F32) * gate_row, axis=1, keepdims=True)
    mix_gate = 1.0 / (1.0 + jnp.exp(-mix_gate))
    for half in range(parts):
        at = pl.ds(2 * part_slots * half, 2 * part_slots)
        packed = dot(pick[at, :rows], normed_two).astype(BF)
        send_rows[pl.ds(part_slots * half, part_slots)] = packed.reshape(part_slots, 2, width)
        exchange(half, send_rows, recv_rows, a_send, a_recv, False)
    recv_rows[own_slot] = send_rows[own_slot]
    t_copies = []
    for k in range(1, GROUP):
        c = pltpu.make_async_remote_copy(
            src_ref=dt.at[0],
            dst_ref=dt.at[k],
            send_sem=t_send.at[k],
            recv_sem=t_recv.at[k],
            device_id=group_peer(k),
            device_id_type=MESH,
        )
        c.start()
        t_copies.append(c)

    pass_on(2)
    pass_on(3)

    for c in late_loads[5:]:
        c.wait()
    others = pl.ds(0, n_ep - 1)
    arrivals = pltpu.make_async_remote_copy(
        src_ref=send_rows.at[others],
        dst_ref=recv_rows.at[others],
        send_sem=a_send,
        recv_sem=a_recv,
        device_id=x_peer(1),
        device_id_type=MESH,
    )
    arrivals.wait_recv()
    routed = recv_rows[...].reshape(n_pick, width)
    hidden = (silu(dot(routed, wg[...])) * dot(routed, wu[...])).astype(BF)
    e_copies = [[], []]
    for k in (2, 1, 3, 0):
        column = pl.ds(pl.multiple_of(lax.rem(tp + k, n_tp) * span, span), span)
        part = dot(hidden, wd[:, column]).astype(BF)
        esend[k] = part.reshape(parts, n_pick // parts, span)
        if k:
            for half in range(parts):
                c = pltpu.make_async_remote_copy(
                    src_ref=esend.at[k, half],
                    dst_ref=erecv.at[k, half],
                    send_sem=e_send.at[k, half],
                    recv_sem=e_recv.at[k, half],
                    device_id=x_peer(k),
                    device_id_type=MESH,
                )
                e_copies[half].append(c)
            e_copies[0][-1].start()
    for c in e_copies[1]:
        c.start()

    for come in (n_z // 2, n_z - (n_z - 1 - n_z // 2)):
        for c in z_copies[come]:
            c.wait_recv()
    for c in t_copies:
        c.wait_recv()
    group_rows = dt[...].reshape(GROUP * rows, width)
    dense_w = n_z * units
    dense_gate = dot_nt(group_rows, gz[:, 0].reshape(dense_w, width))
    dense_up = dot_nt(group_rows, gz[:, 1].reshape(dense_w, width))
    hx[0] = (silu(dense_gate) * dense_up).astype(BF)
    h_copies = []
    for k in (2, 1, 3):
        c = pltpu.make_async_remote_copy(
            src_ref=hx.at[0],
            dst_ref=hx.at[k],
            send_sem=h_send.at[k],
            recv_sem=h_recv.at[k],
            device_id=x_peer(k),
            device_id_type=MESH,
        )
        c.start()
        h_copies.append(c)

    for half in range(parts):
        for c in e_copies[half]:
            c.wait_recv()
        summed = esend[0, half].astype(F32) + erecv[1, half].astype(F32)
        summed = summed + erecv[2, half].astype(F32) + erecv[3, half].astype(F32)
        at = pl.ds(part_slots * half, part_slots)
        back_send[at] = summed.astype(BF).reshape(part_slots, 2, span)
        exchange(half, back_send, back_recv, b_send, b_recv, True)
    back_recv[own_slot] = back_send[own_slot]

    for c in h_copies:
        c.wait_recv()
    dense_part = jnp.zeros((GROUP * rows, span), F32)
    for k in range(n_tp):
        owner = lax.rem(tp + n_tp - k, n_tp)
        part = dz[:, pl.ds(pl.multiple_of(owner * units, units), units), :]
        dense_part = dense_part + dot(hx[k], part.reshape(dense_w, span))
    dsend[...] = dense_part.astype(BF).reshape(GROUP, rows, span)
    d_copies = []
    for k in range(1, GROUP):
        c = pltpu.make_async_remote_copy(
            src_ref=dsend.at[k],
            dst_ref=drecv.at[k],
            send_sem=d_send.at[k],
            recv_sem=d_recv.at[k],
            device_id=group_peer(GROUP - k),
            device_id_type=MESH,
        )
        c.start()
        d_copies.append(c)
    for c in d_copies:
        c.wait_recv()
    dense_sum = dsend[0].astype(F32)
    for k in range(1, GROUP):
        dense_sum = dense_sum + drecv[k].astype(F32)

    returned = pltpu.make_async_remote_copy(
        src_ref=back_send.at[others],
        dst_ref=back_recv.at[others],
        send_sem=b_send,
        recv_sem=b_recv,
        device_id=x_peer(1),
        device_id_type=MESH,
    )
    returned.wait_recv()
    expert_rows = back_recv[...].reshape(n_pick, span)
    expert_sum = dot(comb_hi[:rows], expert_rows) + dot(comb_lo[:rows], expert_rows)
    mine_cols = pl.ds(pl.multiple_of(tp * span, span), span)
    out = resid[:, mine_cols] + expert_sum + mix_gate * dense_sum
    out_ref[...] = out.astype(BF)

    for c in sum(z_copies.values(), []) + x_copies + t_copies + sum(e_copies, []) + h_copies + d_copies:
        c.wait_send()
    arrivals.wait_send()
    returned.wait_send()


def solution(mesh):
    n_ep, n_tp = mesh.shape["ep"], mesh.shape["tp"]

    def shards(*args):
        (
            tokens,
            attn_gain,
            w_query,
            w_key,
            w_value,
            w_forget,
            forget_bias,
            query_gain,
            key_gain,
            cache_pairs,
            cache_cum,
            lengths,
            w_output,
            ffn_gain,
            expert_ids,
            route_weight,
            w_exp_gate,
            w_exp_up,
            w_exp_down,
            shared_gate,
            w_dense_gate,
            w_dense_up,
            w_dense_down,
        ) = args
        rows, width = tokens.shape
        head = query_gain.shape[0]
        slots = cache_pairs.shape[2]
        span = width // n_tp
        n_rows = rows * (w_query.shape[1] // head)
        units = w_dense_gate.shape[0] // n_tp
        n_z = n_ep // GROUP
        ff = w_exp_gate.shape[2]
        n_pick = 2 * n_ep
        operands = (
            tokens,
            attn_gain.reshape(1, -1),
            w_query,
            w_key.T,
            w_value.T,
            w_forget.T,
            forget_bias.reshape(1, -1),
            query_gain.reshape(1, -1),
            key_gain.reshape(1, -1),
            cache_pairs,
            cache_cum,
            lengths.reshape(1, -1),
            w_output,
            ffn_gain.reshape(1, -1),
            expert_ids.T,
            route_weight.T,
            w_exp_gate,
            w_exp_up,
            w_exp_down,
            shared_gate.reshape(-1, 128),
            w_dense_gate,
            w_dense_up,
            w_dense_down,
        )
        dma = pltpu.SemaphoreType.DMA
        vmem = pltpu.VMEM
        like = lambda a: vmem(a.shape, a.dtype)
        scratch = [
            like(tokens),
            like(operands[1]),
            like(w_query),
            like(operands[3]),
            like(operands[4]),
            like(operands[5]),
            like(operands[6]),
            like(operands[7]),
            like(operands[8]),
            vmem((rows, slots, 128), BF),
            like(cache_cum),
            like(operands[11]),
            like(w_output),
            like(operands[13]),
            like(operands[14]),
            like(operands[15]),
            vmem((width, ff), BF),
            vmem((width, ff), BF),
            vmem((ff, width), BF),
            like(operands[19]),
            vmem((n_z, 2, units, width), BF),
            vmem((n_z, units * n_tp, span), BF),
            vmem((rows, slots), F32),
            vmem((n_rows, 256), F32),
            vmem((n_rows, 256), F32),
            vmem((n_rows, slots), F32),
            vmem((n_tp, rows, width), BF),
            vmem((rows, width), F32),
            vmem((GROUP, rows, width), BF),
            vmem((n_ep, 2, width), BF),
            vmem((n_ep, 2, width), BF),
            vmem((n_tp, GROUP * rows, n_z * units), BF),
            vmem((GROUP, rows, span), BF),
            vmem((GROUP, rows, span), BF),
            vmem((n_tp, 2, n_ep, span), BF),
            vmem((n_tp, 2, n_ep, span), BF),
            vmem((n_ep, 2, span), BF),
            vmem((n_ep, 2, span), BF),
            vmem((128, n_pick), BF),
            vmem((128, n_pick), BF),
            vmem((n_pick, 128), BF),
            dma((11,)),
            dma((rows,)),
            dma((8,)),
            dma((3,)),
            dma((2, n_z)),
            dma((2, n_z)),
            dma((n_tp,)),
            dma((n_tp,)),
            dma,
            dma,
            dma((GROUP,)),
            dma((GROUP,)),
            dma((n_tp,)),
            dma((n_tp,)),
            dma((GROUP,)),
            dma((GROUP,)),
            dma((n_tp, 2)),
            dma((n_tp, 2)),
            dma,
            dma,
        ]
        return pl.pallas_call(
            functools.partial(kernel, n_ep, n_tp),
            out_shape=pltpu.VMEM((rows, span), BF),
            in_specs=[pl.BlockSpec(memory_space=pltpu.HBM)] * len(operands),
            out_specs=pl.BlockSpec(memory_space=pltpu.VMEM),
            scratch_shapes=scratch,
            name="layer",
            compiler_params=pltpu.CompilerParams(
                collective_id=0, has_side_effects=True, vmem_limit_bytes=56 * 1024 * 1024
            ),
        )(*operands)

    return jax.shard_map(
        shards,
        mesh=mesh,
        in_specs=(
            P("ep", None),
            P(),
            P(None, "tp"),
            P(None, "tp"),
            P(None, "tp"),
            P(None, "tp"),
            P("tp"),
            P(),
            P(),
            P("ep", "tp", None, None),
            P("ep", "tp", None),
            P("ep"),
            P("tp", None),
            P(),
            P(),
            P(),
            P("ep", None, "tp"),
            P("ep", None, "tp"),
            P("ep", "tp", None),
            P(),
            P("ep", None),
            P("ep", None),
            P("ep", "tp"),
        ),
        out_specs=P("ep", "tp"),
        check_vma=False,
    )
```
